256 devices in a mesh: fs: 16 (over y, x), tp: 16 (over z, core).
Axes of the slice: x: 4, y: 4, z: 8, core: 2. Of those that a mesh axis runs over, the one named last changes fastest.
Arguments:
- tokens: bfloat16 [32768, 2048], P(('fs', 'tp')), may hold values from -24 to 24
- up_gate: bfloat16 [32768, 5632], P('fs', 'tp'), may hold values from -8 to 8
- up_val: bfloat16 [32768, 5632], P('fs', 'tp'), may hold values from -6 to 6
- gate_weight: bfloat16 [2048, 5632], P('fs', 'tp'), may hold values from -0.125 to 0.125
- val_weight: bfloat16 [2048, 5632], P('fs', 'tp'), may hold values from -0.125 to 0.125
- gate_taps: bfloat16 [3, 5632], P(None, 'tp'), may hold values from -3 to 3
- val_taps: bfloat16 [3, 5632], P(None, 'tp'), may hold values from -3 to 3
- hidden_grad: bfloat16 [32768, 5632], P('fs', 'tp'), may hold values from -6 to 6
Outputs:
- input_grad: bfloat16 [32768, 2048], P(('fs', 'tp'))
- gate_weight_grad: float32 [2048, 5632], P('fs', 'tp')
- val_weight_grad: float32 [2048, 5632], P('fs', 'tp')
- gate_taps_grad: float32 [3, 5632], P(None, 'tp')
- val_taps_grad: float32 [3, 5632], P(None, 'tp')
- gate_row_norms: float32 [2048], P('fs')
- val_row_norms: float32 [2048], P('fs')
- tap_row_norms: float32 [2, 3], replicated
The draws below stay inside these ranges and needn't reach their ends.
All inputs are finite; a program needn't handle non-finite values.
Results may differ from the reference program's by a relative error of at most 0.017.
Values may be sent and summed in bfloat16 or wider, within the bound.
A program may use at most 128 MiB of HBM per device.

```python
import jax
import jax.numpy as jnp
from jax import lax

D = 2048
FF = 5632
TAPS = 3
SEQ = 1024
TOKENS = 32768
N_TP = 16


def spiked(entries, stream_key, source, target, parts, factor):
    owner, partner = [(jnp.arange(entries.shape[axis_at]) // (entries.shape[axis_at] // parts)).reshape([-1 if axis == axis_at else 1 for axis in range(entries.ndim)]) for axis_at in (source, target)]
    chosen = jax.random.permutation(stream_key, parts)[partner]
    strong = (owner == chosen) | (owner == (partner + parts // 2) % parts)
    return jnp.where(strong, factor * entries, entries)


def shard_levels(stream_key, dims, shards, smallest, top_value):
    def one(dim, parts):
        steps = jax.random.uniform(jax.random.fold_in(jax.random.fold_in(stream_key, 6), dim), (parts,), jnp.float32, smallest / len(shards), top_value / len(shards))
        return jnp.repeat(jnp.exp(steps), dims[dim] // parts).reshape((-1,) + (1,) * (len(dims) - dim - 1))

    factor_of = one(*shards[0])
    for cut in shards[1:]:
        factor_of = factor_of * one(*cut)
    return factor_of


def scatter_about(rng, shape, width, most, split=(), kind=jnp.bfloat16):
    entries = jax.random.normal(rng, shape, jnp.float32) * width
    if len(split) > 0:
        entries = shard_levels(rng, shape, split, -0.22, 0.18) * entries
    return jnp.clip(entries, min=-most, max=most).astype(kind)


def noise_with(own_key, shape, spread, most, pieces, heavy, kind=jnp.bfloat16):
    drawn = spread * jax.random.normal(own_key, shape, jnp.float32)
    if pieces:
        drawn = drawn * shard_levels(own_key, shape, pieces, -0.22, 0.18)
    return jnp.clip(spiked(drawn, jax.random.fold_in(own_key, 3), *heavy), -most, most).astype(kind)


def setup_inputs(seed: int = 0) -> dict:
    arg_keys = jax.random.split(jax.random.key(seed), 9)
    tokens = noise_with(arg_keys[0], (TOKENS, D), 1.0, 24.0, ((0, 256),), (0, 1, 256, 6.0))
    up_gate = scatter_about(arg_keys[1], (TOKENS, FF), 1.5, 8.0, ((0, 16), (1, 16)))
    up_val = scatter_about(arg_keys[2], (TOKENS, FF), 1.0, 6.0, ((0, 16), (1, 16)))
    gate_weight = scatter_about(arg_keys[3], (D, FF), D ** -0.5, 0.125, ((0, 16), (1, 16)))
    val_weight = scatter_about(arg_keys[4], (D, FF), D ** -0.5, 0.125, ((0, 16), (1, 16)))
    gate_taps = scatter_about(arg_keys[5], (TAPS, FF), 0.6, 3.0, ((1, 16),))
    val_taps = scatter_about(arg_keys[6], (TAPS, FF), 0.6, 3.0, ((1, 16),))
    hidden_grad = noise_with(arg_keys[7], (TOKENS, FF), 1.0, 6.0, ((0, 16), (1, 16)), (0, 1, 16, 2.0))
    return {"tokens": tokens, "up_gate": up_gate, "up_val": up_val, "gate_weight": gate_weight, "val_weight": val_weight, "gate_taps": gate_taps, "val_taps": val_taps, "hidden_grad": hidden_grad}


def shifted_sum(padded, kernel, length, backward):
    tap_count = kernel.shape[0]
    result = jnp.zeros((padded.shape[0], length, padded.shape[2]), jnp.float32)
    for tap_index in range(tap_count):
        tap_shift = tap_count - 1 - tap_index if backward else tap_index
        result = result + kernel[tap_index][None, None, :] * padded[:, tap_shift:tap_shift + length]
    return result


def local_grads(up_gate, up_val, hidden_grad, gate_taps, val_taps):
    length = up_gate.shape[1]
    tap_count = gate_taps.shape[0]
    gate_kernel = gate_taps.astype(jnp.float32)
    val_kernel = val_taps.astype(jnp.float32)
    pad_front = ((0, 0), (tap_count - 1, 0), (0, 0))
    pad_back = ((0, 0), (0, tap_count - 1), (0, 0))
    padded_gate = jnp.pad(up_gate.astype(jnp.float32), pad_front)
    padded_val = jnp.pad(up_val.astype(jnp.float32), pad_front)
    conv_gate = shifted_sum(padded_gate, gate_kernel, length, False)
    conv_val = shifted_sum(padded_val, val_kernel, length, False)
    sigmoid_gate = jax.nn.sigmoid(conv_gate)
    grad_hidden = hidden_grad.astype(jnp.float32)
    val_back = grad_hidden * conv_gate * sigmoid_gate
    gate_back = grad_hidden * conv_val * sigmoid_gate * (1.0 + conv_gate * (1.0 - sigmoid_gate))
    up_gate_back = shifted_sum(jnp.pad(gate_back, pad_back), gate_kernel, length, True).astype(jnp.bfloat16)
    up_val_back = shifted_sum(jnp.pad(val_back, pad_back), val_kernel, length, True).astype(jnp.bfloat16)
    tap_gate = jnp.stack([jnp.sum(padded_gate[:, tap_index:tap_index + length] * gate_back, axis=(0, 1))
                          for tap_index in range(tap_count)])
    tap_val = jnp.stack([jnp.sum(padded_val[:, tap_index:tap_index + length] * val_back, axis=(0, 1))
                         for tap_index in range(tap_count)])
    return up_gate_back, up_val_back, tap_gate, tap_val


def reference(tokens, up_gate, up_val, gate_weight, val_weight, gate_taps, val_taps, hidden_grad):
    width_in = tokens.shape[1]
    hidden_units = up_gate.shape[1]
    block_width = hidden_units // N_TP
    seq_count = tokens.shape[0] // SEQ
    gate_float = gate_weight.astype(jnp.float32).reshape(width_in, N_TP, block_width)
    val_float = val_weight.astype(jnp.float32).reshape(width_in, N_TP, block_width)

    def slice_rows(values, row_start):
        return lax.dynamic_slice_in_dim(values, row_start, SEQ, 0)

    def one_sequence(totals, seq_index):
        row_start = (seq_index * SEQ).astype(jnp.int32)
        local_back = local_grads(slice_rows(up_gate, row_start)[None], slice_rows(up_val, row_start)[None],
                                 slice_rows(hidden_grad, row_start)[None], gate_taps, val_taps)
        gate_back = local_back[0][0]
        val_back = local_back[1][0]
        rows_in = slice_rows(tokens, row_start)
        gate_total = totals[0] + jnp.dot(rows_in.T, gate_back, preferred_element_type=jnp.float32)
        val_total = totals[1] + jnp.dot(rows_in.T, val_back, preferred_element_type=jnp.float32)
        tap_gate_total = totals[2] + local_back[2]
        tap_val_total = totals[3] + local_back[3]
        partials = jnp.einsum('sjf,djf->jsd', gate_back.astype(jnp.float32).reshape(SEQ, N_TP, block_width), gate_float)
        partials = partials + jnp.einsum('sjf,djf->jsd', val_back.astype(jnp.float32).reshape(SEQ, N_TP, block_width), val_float)
        rounded = lax.optimization_barrier(partials.astype(jnp.bfloat16))
        input_rows = jnp.sum(rounded.astype(jnp.float32), axis=0).astype(jnp.bfloat16)
        return (gate_total, val_total, tap_gate_total, tap_val_total), input_rows

    tap_count = gate_taps.shape[0]
    init = (jnp.zeros((width_in, hidden_units), jnp.float32), jnp.zeros((width_in, hidden_units), jnp.float32),
            jnp.zeros((tap_count, hidden_units), jnp.float32), jnp.zeros((tap_count, hidden_units), jnp.float32))
    totals, input_rows = lax.scan(one_sequence, init, jnp.arange(seq_count, dtype=jnp.int32))
    gate_grad, val_grad, tap_gate, tap_val = totals
    input_grad = input_rows.reshape(tokens.shape)
    gate_norms = jnp.sum(gate_grad * gate_grad, axis=1)
    val_norms = jnp.sum(val_grad * val_grad, axis=1)
    tap_norms = jnp.stack([jnp.sum(tap_gate * tap_gate, axis=1), jnp.sum(tap_val * tap_val, axis=1)])
    return (input_grad, gate_grad, val_grad, tap_gate, tap_val, gate_norms, val_norms, tap_norms)
```

```python
import itertools

import jax
import jax.numpy as jnp
from jax import lax
from jax.experimental import pallas as pl
from jax.experimental.pallas import tpu as pltpu
from jax.sharding import Mesh
from jax.sharding import PartitionSpec as P

F32, BF16 = jnp.float32, jnp.bfloat16
MESH = pl.DeviceIdType.MESH
SEQ = 1024
D = 2048
ROWS = 128
WIDTH = 352
WIDE = 384
PAD = 16
CHUNK = 64
NT = (((1,), (1,)), ((), ()))
NN = (((1,), (0,)), ((), ()))
N_COPIES = 106


def kernel(
    tok, ug, uv, gw, vw, gt, vt, hg,
    ig_o, gwg_o, vwg_o, gtg_o, vtg_o, gn_o, vn_o, tn_o,
    TOK, UGI, UVI, HGI, WT, UB, UBT, W, ACC, DA, DB, DA2, DB2,
    RA0, RA1, RB0, RB1, SA0, SA1, SB0, SB1, PB, PX, RS, TX, TY, NC, NZ,
    lsem, ssem, rsem,
):
    y, x, z, c = (lax.axis_index(a) for a in ("y", "x", "z", "c"))
    p = 1 - c

    def ahead(i, k, n):
        return lax.rem(i + k, n)

    ids = itertools.count()
    started = []

    def remote(src, dst, **dev):
        i = next(ids)
        copy = pltpu.make_async_remote_copy(
            src_ref=src, dst_ref=dst, send_sem=ssem.at[i], recv_sem=rsem.at[i],
            device_id=dev, device_id_type=MESH,
        )
        copy.start()
        started.append(copy)
        return copy

    def load(src, dst, i):
        copy = pltpu.make_async_copy(src, dst, lsem.at[i])
        copy.start()
        return copy

    own_rows = pl.ds(pl.multiple_of(c * ROWS, ROWS), ROWS)
    l_tok = load(tok, TOK.at[z, own_rows], 0)
    l_gw = load(gw, WT.at[0], 1)
    l_vw = load(vw, WT.at[1], 2)
    l_in = []
    for s in range(2):
        at = pl.ds(s * SEQ, SEQ)
        l_in.append(
            (
                load(ug.at[at], UGI.at[s, pl.ds(PAD, SEQ)], 3 + 3 * s),
                load(uv.at[at], UVI.at[s, pl.ds(PAD, SEQ)], 4 + 3 * s),
                load(hg.at[at], HGI.at[s], 5 + 3 * s),
            )
        )

    barrier = pltpu.get_barrier_semaphore()
    peers = [{"c": p}]
    peers += [{"x": ahead(x, k, 4)} for k in (1, 2, 3)]
    peers += [{"y": ahead(y, k, 4)} for k in (1, 2, 3)]
    peers += [{"z": ahead(z, k, 8)} for k in range(1, 8)]
    for peer in peers:
        pl.semaphore_signal(barrier, inc=1, device_id=peer, device_id_type=MESH)

    l_gw.wait()
    l_vw.wait()
    W[y, x] = jnp.zeros((ROWS, 2 * WIDE), BF16)
    W[y, x, :, 0:WIDTH] = WT[0]
    W[y, x, :, WIDE : WIDE + WIDTH] = WT[1]
    l_tok.wait()
    pl.semaphore_wait(barrier, len(peers))

    def tok_at(zz, core, h):
        return TOK.at[zz, pl.ds(pl.multiple_of(core * ROWS + h * 64, 64), 64)]

    order_up = [(0, 0), (0, 1), (1, 0), (1, 1), (2, 0), (2, 1), (3, 0)]
    order_dn = [(s, 1 - h) for s, h in order_up]
    up, down, cross = {}, {}, {}

    def tok_send(j):
        s, h = order_up[j]
        blk = tok_at(ahead(z, 8 - s, 8), c, h)
        up[j] = remote(blk, blk, z=ahead(z, 1, 8))
        s, h = order_dn[j]
        blk = tok_at(ahead(z, s, 8), c, h)
        down[j] = remote(blk, blk, z=ahead(z, 7, 8))

    def tok_cross(k, h):
        blk = tok_at(ahead(z, k, 8), c, h)
        cross[k, h] = remote(blk, blk, c=p)

    def tok_event(j):
        up[j].wait_recv()
        down[j].wait_recv()
        if j + 2 < 7:
            tok_send(j + 2)
        s, h = order_up[j]
        tok_cross(7 - s, h)
        s, h = order_dn[j]
        tok_cross(1 + s, h)

    tok_send(0)
    tok_send(1)
    tok_cross(0, 0)
    tok_cross(0, 1)

    def gather(slot, axis, i):
        state = {}

        def begin():
            for d, s in ((0, 1), (1, 3)):
                state[d] = remote(slot(i, None), slot(i, None), **{axis: ahead(i, s, 4)})

        def middle():
            for d, s in ((0, 1), (1, 3)):
                state[d].wait_recv()
                far = ahead(i, 4 - s, 4)
                state[2 + d] = remote(slot(far, d), slot(far, d), **{axis: ahead(i, s, 4)})

        def end():
            state[2].wait_recv()
            state[3].wait_recv()

        return begin, middle, end

    def a1(i, d):
        return W.at[y, i, pl.ds(0, 64) if d is None else pl.ds(32 * d, 32)]

    def b1(i, d):
        return W.at[i, x, pl.ds(64, 64) if d is None else pl.ds(64 + 32 * d, 32)]

    def a2(i, d):
        return W.at[i, pl.ds(0, 4) if d is None else pl.ds(2 * d, 2), pl.ds(0, 64)]

    def b2(i, d):
        return W.at[pl.ds(0, 4) if d is None else pl.ds(2 * d, 2), i, pl.ds(64, 64)]

    first = gather(a1, "x", x), gather(b1, "y", y)
    second = gather(a2, "y", y), gather(b2, "x", x)
    for g in first:
        g[0]()

    for s in range(2):
        UGI[s, 0:PAD] = jnp.zeros((PAD, WIDTH), BF16)
        UVI[s, 0:PAD] = jnp.zeros((PAD, WIDTH), BF16)
    UB[:, 256:384] = jnp.zeros((2 * SEQ, 128), BF16)
    UB[:, 640:768] = jnp.zeros((2 * SEQ, 128), BF16)
    TX[x] = jnp.zeros((2, 8, WIDE), F32)

    def conv(s, t):
        lo, hi = t * 128, min(t * 128 + 128, WIDTH)
        n = hi - lo
        kg = [gt[i : i + 1, lo:hi].astype(F32) for i in range(3)]
        kv = [vt[i : i + 1, lo:hi].astype(F32) for i in range(3)]

        def fold(a):
            return jnp.sum(a.reshape(CHUNK // 8, 8, n), axis=0)

        def step(j, carry):
            sums, gb_next, vb_next = carry
            r = pl.multiple_of((SEQ // CHUNK - 1 - j) * CHUNK, CHUNK)
            g = UGI[s, pl.ds(r, CHUNK + PAD), lo:hi].astype(F32)
            v = UVI[s, pl.ds(r, CHUNK + PAD), lo:hi].astype(F32)
            h = HGI[s, pl.ds(r, CHUNK), lo:hi].astype(F32)
            gs = [g[PAD - 2 + i : PAD - 2 + i + CHUNK] for i in range(3)]
            vs = [v[PAD - 2 + i : PAD - 2 + i + CHUNK] for i in range(3)]
            cg = kg[0] * gs[0] + kg[1] * gs[1] + kg[2] * gs[2]
            cv = kv[0] * vs[0] + kv[1] * vs[1] + kv[2] * vs[2]
            sg = jax.nn.sigmoid(cg)
            hs = h * sg
            vb = hs * cg
            gb = hs * cv * (1.0 + cg * (1.0 - sg))
            sums = tuple(
                a + fold(b)
                for a, b in zip(sums, [u * gb for u in gs] + [u * vb for u in vs])
            )
            gx = jnp.concatenate([gb, gb_next], axis=0)
            vx = jnp.concatenate([vb, vb_next], axis=0)
            og = kg[2] * gb + kg[1] * gx[1 : CHUNK + 1] + kg[0] * gx[2 : CHUNK + 2]
            ov = kv[2] * vb + kv[1] * vx[1 : CHUNK + 1] + kv[0] * vx[2 : CHUNK + 2]
            at = pl.ds(s * SEQ + r, CHUNK)
            UB[at, lo:hi] = og.astype(BF16)
            UB[at, WIDE + lo : WIDE + hi] = ov.astype(BF16)
            return sums, gb[0:8], vb[0:8]

        zero = jnp.zeros((8, n), F32)
        sums, _, _ = lax.fori_loop(0, SEQ // CHUNK, step, ((zero,) * 6, zero, zero))
        for i in range(3):
            for q in range(2):
                TX[x, q, i : i + 1, lo:hi] += jnp.sum(sums[3 * q + i], axis=0, keepdims=True)

    def turn(zz):
        for t in range(6):
            UBT[zz, t * 128 : t * 128 + 128, :] = UB[
                pl.ds(pl.multiple_of(zz * 256, 256), 256), t * 128 : t * 128 + 128
            ].T

    def weight_part(ks, first_part=False, last_part=False):
        zs = [ahead(z, k, 8) for k in ks]

        def step(n, _):
            cols = pl.ds(pl.multiple_of(n * 256, 256), 256)
            total = None
            for zz in zs:
                part = lax.dot_general(UBT[zz], TOK[zz, :, cols], NN, preferred_element_type=F32)
                total = part if total is None else total + part
            if not first_part:
                total = total + ACC[n]
            if last_part:
                out = total.astype(BF16)
                yy, xx = n // 2, 2 * (n % 2)
                for q in range(2):
                    DA[xx + q, yy // 2, yy % 2] = out[0:WIDE, q * 128 : q * 128 + 128]
                    DB[yy, xx // 2, q] = out[WIDE : 2 * WIDE, q * 128 : q * 128 + 128]
            else:
                ACC[n] = total
            return 0

        lax.fori_loop(0, 8, step, 0)

    def wait_cross(*ks):
        for k in ks:
            cross[k, 0].wait_recv()
            cross[k, 1].wait_recv()

    partner = {}

    def input_part(k):
        zz = ahead(z, k, 8)
        rows = pl.ds(pl.multiple_of(zz * 256, 256), 256)

        def step(n, _):
            w = W[n // 2, pl.ds(2 * (n % 2), 2)].reshape(256, 2 * WIDE)
            out = lax.dot_general(UB[rows, :], w, NT, preferred_element_type=F32).astype(BF16)
            cols = pl.ds(pl.multiple_of(n * 256, 256), 256)
            PB[k, 0, :, cols] = out[0:128]
            PB[k, 1, :, cols] = out[128:256]
            return 0

        lax.fori_loop(0, 8, step, 0)
        partner[k] = remote(PB.at[k, p], PX.at[k], c=p)

    sum_up = [(0, 0), (1, 1), (1, 0), (2, 1), (2, 0), (3, 1), (3, 0)]
    flow = {}

    def pair_sum(k, h, extra):
        def step(i, _):
            rows = pl.ds(pl.multiple_of(h * 64 + i * 16, 16), 16)
            v = PB[k, c, rows, :].astype(F32) + PX[k, rows, :].astype(F32)
            if extra is not None:
                v = v + RS[extra[0], extra[1], pl.ds(pl.multiple_of(i * 16, 16), 16), :].astype(F32)
            PB[k, c, rows, :] = v.astype(BF16)
            return 0

        lax.fori_loop(0, 4, step, 0)

    def sum_event(j):
        for d in range(2):
            s, h = sum_up[j]
            if d:
                h = 1 - h
            k = 4 - s if d == 0 else 4 + s
            if j == 0 and d == 0 or j == 1 or j == 3 or j == 5:
                partner[k].wait_recv()
            if j >= 2:
                flow[d, j - 2].wait_recv()
            pair_sum(k, h, (d, j - 2) if j >= 2 else None)
            flow[d, j] = remote(
                PB.at[k, c, pl.ds(h * 64, 64)], RS.at[d, j], z=ahead(z, 1 if d == 0 else 7, 8)
            )

    def scatter(src, r0, r1, axis, i):
        state = {}
        own = i
        near = {0: ahead(i, 1, 4), 1: ahead(i, 3, 4)}
        far = ahead(i, 2, 4)

        def begin():
            for d in range(2):
                to = {axis: near[d]}
                state[d] = remote(src.at[far, d], r0.at[d], **to)
                state[2 + d] = remote(src.at[near[d], 1 - d], r1.at[d, 1 - d], **to)

        def middle():
            for d in range(2):
                state[d].wait_recv()
                src[near[d], d] = (src[near[d], d].astype(F32) + r0[d].astype(F32)).astype(BF16)
                state[4 + d] = remote(src.at[near[d], d], r1.at[d, d], **{axis: near[d]})

        def end():
            for i_ in range(2, 6):
                state[i_].wait_recv()

        def total(*at):
            t = src[(own, *at)].astype(F32)
            return t + r1[(0, *at)].astype(F32) + r1[(1, *at)].astype(F32)

        return begin, middle, end, total

    sc_a1 = scatter(DA, RA0, RA1, "x", x)
    sc_b1 = scatter(DB, RB0, RB1, "y", y)
    sc_a2 = scatter(DA2, SA0, SA1, "y", y)
    sc_b2 = scatter(DB2, SB0, SB1, "x", x)

    def tap_sum(ref):
        return ref[0] + ref[1] + ref[2] + ref[3]

    for s in range(2):
        for copy in l_in[s]:
            copy.wait()
        for t in range(3):
            conv(s, t)
            if s == 0 and t == 1:
                for g in first:
                    g[1]()
            if s == 1 and t == 0:
                for g in first:
                    g[2]()
                for g in second:
                    g[0]()
    tap_x = [remote(TX.at[x], TX.at[x], x=ahead(x, k, 4)) for k in (1, 2, 3)]
    tok_event(0)
    lax.fori_loop(0, 8, lambda i, _: (turn(i), 0)[1], 0)
    tok_event(1)
    for copy in tap_x:
        copy.wait_recv()
    TY[y] = tap_sum(TX)
    tap_y = [remote(TY.at[y], TY.at[y], y=ahead(y, k, 4)) for k in (1, 2, 3)]
    wait_cross(0)
    weight_part([0], first_part=True)
    tok_event(2)
    for g in second:
        g[1]()
    wait_cross(1, 7)
    weight_part([1, 7])
    tok_event(3)
    for copy in tap_y:
        copy.wait_recv()
    taps = tap_sum(TY)
    gtg_o[...] = taps[0, 0:3, 0:WIDTH]
    vtg_o[...] = taps[1, 0:3, 0:WIDTH]
    NC[c, 1] = jnp.broadcast_to(jnp.sum(taps[0] * taps[0], axis=1, keepdims=True), (8, 128))
    NC[c, 2] = jnp.broadcast_to(jnp.sum(taps[1] * taps[1], axis=1, keepdims=True), (8, 128))
    tok_event(4)
    for g in second:
        g[2]()
    input_part(4)
    input_part(3)
    input_part(5)
    tok_event(5)
    sum_event(0)
    sum_event(1)
    wait_cross(2, 6)
    weight_part([2, 6])
    tok_event(6)
    wait_cross(3, 5)
    weight_part([3, 5])
    wait_cross(4)
    weight_part([4], last_part=True)
    sc_a1[0]()
    sc_b1[0]()
    input_part(2)
    input_part(6)
    sum_event(2)
    input_part(1)
    sum_event(3)
    sc_a1[1]()
    sc_b1[1]()
    input_part(7)
    sum_event(4)
    input_part(0)
    sc_a1[2]()
    sc_b1[2]()
    for q in range(4):
        DA2[q] = sc_a1[3](q // 2, q % 2).astype(BF16).reshape(2, 192, 128)
        DB2[q] = sc_b1[3](q // 2, q % 2).astype(BF16).reshape(2, 192, 128)
    sc_a2[0]()
    sc_b2[0]()
    sum_event(5)
    sc_a2[1]()
    sc_b2[1]()
    sum_event(6)
    sc_a2[2]()
    sc_b2[2]()
    norms = []
    for scat, out in ((sc_a2, gwg_o), (sc_b2, vwg_o)):
        grad = scat[3]().reshape(WIDE, 128)
        norms.append(jnp.sum(grad * grad, axis=0, keepdims=True))
        out[...] = grad.T[:, 0:WIDTH]
    NC[c, 0, 0:1] = norms[0]
    NC[c, 0, 1:2] = norms[1]
    pair = remote(NC.at[c], NC.at[c], c=p)
    pair.wait_recv()
    NZ[z] = NC[0] + NC[1]
    along = [remote(NZ.at[z], NZ.at[z], z=ahead(z, k, 8)) for k in range(1, 8)]
    partner[0].wait_recv()
    for d in range(2):
        flow[d, 5].wait_recv()
        flow[d, 6].wait_recv()

    for h in range(2):
        j_up = 6 if h == 0 else 5
        j_dn = 5 if h == 0 else 6

        def step(i, _, h=h, j_up=j_up, j_dn=j_dn):
            rows = pl.ds(pl.multiple_of(h * 64 + i * 16, 16), 16)
            here = pl.ds(pl.multiple_of(i * 16, 16), 16)
            v = PB[0, c, rows, :].astype(F32) + PX[0, rows, :].astype(F32)
            v = v + RS[0, j_up, here, :].astype(F32) + RS[1, j_dn, here, :].astype(F32)
            ig_o[rows, :] = v.astype(BF16)
            return 0

        lax.fori_loop(0, 4, step, 0)

    for copy in along:
        copy.wait_recv()
    total = NZ[0]
    for k in range(1, 8):
        total = total + NZ[k]
    gn_o[...] = total[0, 0:1]
    vn_o[...] = total[0, 1:2]
    diagonal = lax.broadcasted_iota(jnp.int32, (8, 128), 0) == lax.broadcasted_iota(
        jnp.int32, (8, 128), 1
    )
    for q in range(2):
        row = jnp.sum(jnp.where(diagonal, total[1 + q], 0.0), axis=0, keepdims=True)
        tn_o[q : q + 1, :] = row[:, 0:3]
    for copy in started:
        copy.wait_send()
    assert len(started) == N_COPIES, len(started)


def local(tokens, up_gate, up_val, gate_weight, val_weight, gate_taps, val_taps, hidden_grad):
    hbm = pl.BlockSpec(memory_space=pl.ANY)
    vmem = pl.BlockSpec(memory_space=pltpu.VMEM)
    half = WIDE // 2
    scratch = [
        pltpu.VMEM((8, 256, D), BF16),
        pltpu.VMEM((2, PAD + SEQ, WIDTH), BF16),
        pltpu.VMEM((2, PAD + SEQ, WIDTH), BF16),
        pltpu.VMEM((2, SEQ, WIDTH), BF16),
        pltpu.VMEM((2, ROWS, WIDTH), BF16),
        pltpu.VMEM((2 * SEQ, 2 * WIDE), BF16),
        pltpu.VMEM((8, 2 * WIDE, 256), BF16),
        pltpu.VMEM((4, 4, ROWS, 2 * WIDE), BF16),
        pltpu.VMEM((8, 2 * WIDE, 256), F32),
        pltpu.VMEM((4, 2, 2, WIDE, 128), BF16),
        pltpu.VMEM((4, 2, 2, WIDE, 128), BF16),
        pltpu.VMEM((4, 2, half, 128), BF16),
        pltpu.VMEM((4, 2, half, 128), BF16),
        pltpu.VMEM((2, 2, WIDE, 128), BF16),
        pltpu.VMEM((2, 2, 2, WIDE, 128), BF16),
        pltpu.VMEM((2, 2, WIDE, 128), BF16),
        pltpu.VMEM((2, 2, 2, WIDE, 128), BF16),
        pltpu.VMEM((2, half, 128), BF16),
        pltpu.VMEM((2, 2, half, 128), BF16),
        pltpu.VMEM((2, half, 128), BF16),
        pltpu.VMEM((2, 2, half, 128), BF16),
        pltpu.VMEM((8, 2, ROWS, D), BF16),
        pltpu.VMEM((8, ROWS, D), BF16),
        pltpu.VMEM((2, 7, 64, D), BF16),
        pltpu.VMEM((4, 2, 8, WIDE), F32),
        pltpu.VMEM((4, 2, 8, WIDE), F32),
        pltpu.VMEM((2, 3, 8, 128), F32),
        pltpu.VMEM((8, 3, 8, 128), F32),
        pltpu.SemaphoreType.DMA((9,)),
        pltpu.SemaphoreType.DMA((N_COPIES,)),
        pltpu.SemaphoreType.DMA((N_COPIES,)),
    ]
    out = pl.pallas_call(
        kernel,
        out_shape=[
            jax.ShapeDtypeStruct((ROWS, D), BF16),
            jax.ShapeDtypeStruct((ROWS, WIDTH), F32),
            jax.ShapeDtypeStruct((ROWS, WIDTH), F32),
            jax.ShapeDtypeStruct((3, WIDTH), F32),
            jax.ShapeDtypeStruct((3, WIDTH), F32),
            jax.ShapeDtypeStruct((1, ROWS), F32),
            jax.ShapeDtypeStruct((1, ROWS), F32),
            jax.ShapeDtypeStruct((2, 3), F32),
        ],
        in_specs=[hbm, hbm, hbm, hbm, hbm, vmem, vmem, hbm],
        out_specs=[vmem] * 8,
        scratch_shapes=scratch,
        compiler_params=pltpu.CompilerParams(
            collective_id=0, has_side_effects=True, vmem_limit_bytes=67_000_000
        ),
        name="backward",
    )(tokens, up_gate, up_val, gate_weight, val_weight, gate_taps, val_taps, hidden_grad)
    return (*out[:5], out[5].reshape(ROWS), out[6].reshape(ROWS), out[7])


def solution(mesh):
    split = Mesh(mesh.devices.reshape(4, 4, 8, 2), ("y", "x", "z", "c"))
    fs, tp, both = ("y", "x"), ("z", "c"), ("y", "x", "z", "c")
    in_specs = (
        P(both, None), P(fs, tp), P(fs, tp), P(fs, tp), P(fs, tp), P(None, tp), P(None, tp), P(fs, tp),
    )
    out_specs = (
        P(both, None), P(fs, tp), P(fs, tp), P(None, tp), P(None, tp), P(fs), P(fs), P(),
    )
    return jax.shard_map(local, mesh=split, in_specs=in_specs, out_specs=out_specs, check_vma=False)
```

```python
import itertools

import jax
import jax.numpy as jnp
from jax import lax
from jax.experimental import pallas as pl
from jax.experimental.pallas import tpu as pltpu
from jax.sharding import Mesh
from jax.sharding import PartitionSpec as P

F32, BF16 = jnp.float32, jnp.bfloat16
MESH = pl.DeviceIdType.MESH
SEQ = 1024
D = 2048
ROWS = 128
WIDTH = 352
BOTH = 2 * WIDTH
GROUP = 16
TILES = SEQ // 128
NN = (((1,), (0,)), ((), ()))
N_COPIES = 106


def kernel(
    tok, ug, uv, gw, vw, gt, vt, hg,
    ig_o, gwg_o, vwg_o, gtg_o, vtg_o, gn_o, vn_o, tn_o,
    TOK, UGI, UVI, HGI, KT, TS, UB, UBT, W, ACC, DA, DB, DA2, DB2,
    RA0, RA1, RB0, RB1, SA0, SA1, SB0, SB1, PB, PX, RS, TX, TY, NC, NZ,
    lsem, ssem, rsem,
):
    y, x, z, c = (lax.axis_index(a) for a in ("y", "x", "z", "c"))
    p = 1 - c

    def ahead(i, k, n):
        return lax.rem(i + k, n)

    ids = itertools.count()
    started = []

    def remote(src, dst, **dev):
        i = next(ids)
        copy = pltpu.make_async_remote_copy(
            src_ref=src, dst_ref=dst, send_sem=ssem.at[i], recv_sem=rsem.at[i],
            device_id=dev, device_id_type=MESH,
        )
        copy.start()
        started.append(copy)
        return copy

    def load(src, dst, i):
        copy = pltpu.make_async_copy(src, dst, lsem.at[i])
        copy.start()
        return copy

    own_rows = pl.ds(pl.multiple_of(c * ROWS, ROWS), ROWS)
    l_tok = load(tok, TOK.at[z, own_rows], 0)
    l_gw = load(gw, W.at[y, x, pl.ds(0, WIDTH)], 1)
    l_vw = load(vw, W.at[y, x, pl.ds(WIDTH, WIDTH)], 2)
    l_in = [load(a, b, 3 + i) for i, (a, b) in enumerate(((ug, UGI), (uv, UVI), (hg, HGI)))]

    barrier = pltpu.get_barrier_semaphore()
    peers = [{"c": p}]
    peers += [{"x": ahead(x, k, 4)} for k in (1, 2, 3)]
    peers += [{"y": ahead(y, k, 4)} for k in (1, 2, 3)]
    peers += [{"z": ahead(z, k, 8)} for k in range(1, 8)]
    for peer in peers:
        pl.semaphore_signal(barrier, inc=1, device_id=peer, device_id_type=MESH)

    l_tok.wait()
    pl.semaphore_wait(barrier, len(peers))

    def tok_at(zz, core, h):
        return TOK.at[zz, pl.ds(pl.multiple_of(core * ROWS + h * 64, 64), 64)]

    order_up = [(0, 0), (0, 1), (1, 0), (1, 1), (2, 0), (2, 1), (3, 0)]
    order_dn = [(s, 1 - h) for s, h in order_up]
    up, down, cross = {}, {}, {}

    def tok_send(j):
        s, h = order_up[j]
        blk = tok_at(ahead(z, 8 - s, 8), c, h)
        up[j] = remote(blk, blk, z=ahead(z, 1, 8))
        s, h = order_dn[j]
        blk = tok_at(ahead(z, s, 8), c, h)
        down[j] = remote(blk, blk, z=ahead(z, 7, 8))

    def tok_cross(k, h):
        blk = tok_at(ahead(z, k, 8), c, h)
        cross[k, h] = remote(blk, blk, c=p)

    def tok_event(j):
        up[j].wait_recv()
        down[j].wait_recv()
        if j + 2 < 7:
            tok_send(j + 2)
        s, h = order_up[j]
        tok_cross(7 - s, h)
        s, h = order_dn[j]
        tok_cross(1 + s, h)

    tok_send(0)
    tok_send(1)
    tok_cross(0, 0)
    tok_cross(0, 1)

    def gather(slot, axis, i):
        state = {}

        def begin():
            for d, s in ((0, 1), (1, 3)):
                state[d] = remote(slot(i, None), slot(i, None), **{axis: ahead(i, s, 4)})

        def middle():
            for d, s in ((0, 1), (1, 3)):
                state[d].wait_recv()
                far = ahead(i, 4 - s, 4)
                state[2 + d] = remote(slot(far, d), slot(far, d), **{axis: ahead(i, s, 4)})

        def end():
            state[2].wait_recv()
            state[3].wait_recv()

        return begin, middle, end

    quarter = WIDTH // 2

    def a1(i, d):
        return W.at[y, i, pl.ds(0, WIDTH) if d is None else pl.ds(quarter * d, quarter)]

    def b1(i, d):
        rows = pl.ds(WIDTH, WIDTH) if d is None else pl.ds(WIDTH + quarter * d, quarter)
        return W.at[i, x, rows]

    def a2(i, d):
        return W.at[i, pl.ds(0, 4) if d is None else pl.ds(2 * d, 2), pl.ds(0, WIDTH)]

    def b2(i, d):
        return W.at[pl.ds(0, 4) if d is None else pl.ds(2 * d, 2), i, pl.ds(WIDTH, WIDTH)]

    first = gather(a1, "x", x), gather(b1, "y", y)
    second = gather(a2, "y", y), gather(b2, "x", x)
    l_gw.wait()
    l_vw.wait()
    for g in first:
        g[0]()

    for q, ref in enumerate((gt, vt)):
        rows = jnp.concatenate([ref[...].astype(F32), jnp.zeros((5, WIDTH), F32)], axis=0)
        for t in range(3):
            lo, hi = t * 128, min(t * 128 + 128, WIDTH)
            KT[q, lo:hi, 0:8] = rows[:, lo:hi].T

    lane = lax.broadcasted_iota(jnp.int32, (GROUP, 128), 1)
    edge = {1: lane >= 1, 2: lane >= 2, -1: lane < 127, -2: lane < 126}
    nil = jnp.zeros((GROUP, 128), F32)

    def moved(tiles, k):
        turned = [pltpu.roll(a, k % 128, 1) for a in tiles]
        if k > 0:
            other = [nil] + turned[:-1]
        else:
            other = turned[1:] + [nil]
        return [jnp.where(edge[k], a, b) for a, b in zip(turned, other)]

    def conv(first_group, last_group):
        def step(g, _):
            rows = pl.ds(pl.multiple_of(g * GROUP, GROUP), GROUP)
            low = pl.ds(pl.multiple_of(WIDTH + g * GROUP, GROUP), GROUP)
            kg = [jnp.broadcast_to(KT[0, rows, i : i + 1], (GROUP, 128)) for i in range(3)]
            kv = [jnp.broadcast_to(KT[1, rows, i : i + 1], (GROUP, 128)) for i in range(3)]
            sums = [nil] * 6
            for s in range(2):
                at = [slice(s * SEQ + i * 128, s * SEQ + i * 128 + 128) for i in range(TILES)]
                g0 = [UGI[rows, a].astype(F32) for a in at]
                v0 = [UVI[rows, a].astype(F32) for a in at]
                g1, g2, v1, v2 = moved(g0, 1), moved(g0, 2), moved(v0, 1), moved(v0, 2)
                gb, vb = [], []
                for i in range(TILES):
                    h = HGI[rows, at[i]].astype(F32)
                    cg = kg[0] * g2[i] + kg[1] * g1[i] + kg[2] * g0[i]
                    cv = kv[0] * v2[i] + kv[1] * v1[i] + kv[2] * v0[i]
                    sg = jax.nn.sigmoid(cg)
                    hs = h * sg
                    vb.append(hs * cg)
                    gb.append(hs * cv * (1.0 + cg * (1.0 - sg)))
                    terms = [u * gb[i] for u in (g2[i], g1[i], g0[i])]
                    terms += [u * vb[i] for u in (v2[i], v1[i], v0[i])]
                    sums = [a + b for a, b in zip(sums, terms)]
                gb1, gb2, vb1, vb2 = moved(gb, -1), moved(gb, -2), moved(vb, -1), moved(vb, -2)
                for i in range(TILES):
                    half = slice((i % 2) * 128, (i % 2) * 128 + 128)
                    og = kg[2] * gb[i] + kg[1] * gb1[i] + kg[0] * gb2[i]
                    ov = kv[2] * vb[i] + kv[1] * vb1[i] + kv[0] * vb2[i]
                    UBT[4 * s + i // 2, rows, half] = og.astype(BF16)
                    UBT[4 * s + i // 2, low, half] = ov.astype(BF16)
            for q in range(2):
                t = [jnp.sum(sums[3 * q + i], axis=1, keepdims=True) for i in range(3)]
                TS[q, rows, :] = jnp.where(
                    lane == 0, t[0], jnp.where(lane == 1, t[1], jnp.where(lane == 2, t[2], 0.0))
                )
            return 0

        lax.fori_loop(first_group, last_group, step, 0)

    def turn(zz):
        rows = pl.ds(pl.multiple_of(zz * 256, 256), 256)
        for lo in range(0, BOTH, 128):
            hi = min(lo + 128, BOTH)
            UB[rows, lo:hi] = UBT[zz, lo:hi, :].T

    def weight_part(ks, first_part=False, last_part=False):
        zs = [ahead(z, k, 8) for k in ks]

        def step(n, _):
            cols = pl.ds(pl.multiple_of(n * 256, 256), 256)
            total = None
            for zz in zs:
                part = lax.dot_general(UBT[zz], TOK[zz, :, cols], NN, preferred_element_type=F32)
                total = part if total is None else total + part
            if not first_part:
                total = total + ACC[n]
            if last_part:
                out = total.astype(BF16)
                yy, xx = n // 2, 2 * (n % 2)
                for q in range(2):
                    DA[xx + q, yy // 2, yy % 2] = out[0:WIDTH, q * 128 : q * 128 + 128]
                    DB[yy, xx // 2, q] = out[WIDTH:BOTH, q * 128 : q * 128 + 128]
            else:
                ACC[n] = total
            return 0

        lax.fori_loop(0, 8, step, 0)

    def wait_cross(*ks):
        for k in ks:
            cross[k, 0].wait_recv()
            cross[k, 1].wait_recv()

    partner = {}

    def input_part(k):
        zz = ahead(z, k, 8)
        rows = pl.ds(pl.multiple_of(zz * 256, 256), 256)

        def step(n, _):
            yy, xx = n // 2, 2 * (n % 2)
            w = jnp.concatenate([W[yy, xx], W[yy, xx + 1]], axis=1)
            out = lax.dot_general(UB[rows, :], w, NN, preferred_element_type=F32).astype(BF16)
            cols = pl.ds(pl.multiple_of(n * 256, 256), 256)
            PB[k, 0, :, cols] = out[0:128]
            PB[k, 1, :, cols] = out[128:256]
            return 0

        lax.fori_loop(0, 8, step, 0)
        partner[k] = remote(PB.at[k, p], PX.at[k], c=p)

    sum_up = [(0, 0), (1, 1), (1, 0), (2, 1), (2, 0), (3, 1), (3, 0)]
    flow = {}

    def pair_sum(k, h, extra):
        def step(i, _):
            rows = pl.ds(pl.multiple_of(h * 64 + i * 16, 16), 16)
            v = PB[k, c, rows, :].astype(F32) + PX[k, rows, :].astype(F32)
            if extra is not None:
                v = v + RS[extra[0], extra[1], pl.ds(pl.multiple_of(i * 16, 16), 16), :].astype(F32)
            PB[k, c, rows, :] = v.astype(BF16)
            return 0

        lax.fori_loop(0, 4, step, 0)

    def sum_event(j):
        for d in range(2):
            s, h = sum_up[j]
            if d:
                h = 1 - h
            k = 4 - s if d == 0 else 4 + s
            if j == 0 and d == 0 or j == 1 or j == 3 or j == 5:
                partner[k].wait_recv()
            if j >= 2:
                flow[d, j - 2].wait_recv()
            pair_sum(k, h, (d, j - 2) if j >= 2 else None)
            flow[d, j] = remote(
                PB.at[k, c, pl.ds(h * 64, 64)], RS.at[d, j], z=ahead(z, 1 if d == 0 else 7, 8)
            )

    def scatter(src, r0, r1, axis, i):
        state = {}
        own = i
        near = {0: ahead(i, 1, 4), 1: ahead(i, 3, 4)}
        far = ahead(i, 2, 4)

        def begin():
            for d in range(2):
                to = {axis: near[d]}
                state[d] = remote(src.at[far, d], r0.at[d], **to)
                state[2 + d] = remote(src.at[near[d], 1 - d], r1.at[d, 1 - d], **to)

        def middle():
            for d in range(2):
                state[d].wait_recv()
                src[near[d], d] = (src[near[d], d].astype(F32) + r0[d].astype(F32)).astype(BF16)
                state[4 + d] = remote(src.at[near[d], d], r1.at[d, d], **{axis: near[d]})

        def end():
            for i_ in range(2, 6):
                state[i_].wait_recv()

        def total(*at):
            t = src[(own, *at)].astype(F32)
            return t + r1[(0, *at)].astype(F32) + r1[(1, *at)].astype(F32)

        return begin, middle, end, total

    sc_a1 = scatter(DA, RA0, RA1, "x", x)
    sc_b1 = scatter(DB, RB0, RB1, "y", y)
    sc_a2 = scatter(DA2, SA0, SA1, "y", y)
    sc_b2 = scatter(DB2, SB0, SB1, "x", x)

    def tap_sum(ref):
        return ref[0] + ref[1] + ref[2] + ref[3]

    for copy in l_in:
        copy.wait()
    conv(0, 8)
    for g in first:
        g[1]()
    conv(8, 16)
    for g in first:
        g[2]()
    for g in second:
        g[0]()
    conv(16, 22)
    for q in range(2):
        for lo in range(0, WIDTH, 128):
            hi = min(lo + 128, WIDTH)
            TX[x, q, :, lo:hi] = TS[q, lo:hi, :].T[0:8]
    tap_x = [remote(TX.at[x], TX.at[x], x=ahead(x, k, 4)) for k in (1, 2, 3)]
    tok_event(0)
    lax.fori_loop(0, 8, lambda i, _: (turn(i), 0)[1], 0)
    tok_event(1)
    for copy in tap_x:
        copy.wait_recv()
    TY[y] = tap_sum(TX)
    tap_y = [remote(TY.at[y], TY.at[y], y=ahead(y, k, 4)) for k in (1, 2, 3)]
    wait_cross(0)
    weight_part([0], first_part=True)
    tok_event(2)
    for g in second:
        g[1]()
    wait_cross(1, 7)
    weight_part([1, 7])
    tok_event(3)
    for copy in tap_y:
        copy.wait_recv()
    taps = tap_sum(TY)
    gtg_o[...] = taps[0, 0:3, 0:WIDTH]
    vtg_o[...] = taps[1, 0:3, 0:WIDTH]
    NC[c, 1] = jnp.broadcast_to(jnp.sum(taps[0] * taps[0], axis=1, keepdims=True), (8, 128))
    NC[c, 2] = jnp.broadcast_to(jnp.sum(taps[1] * taps[1], axis=1, keepdims=True), (8, 128))
    tok_event(4)
    for g in second:
        g[2]()
    input_part(4)
    input_part(3)
    input_part(5)
    tok_event(5)
    sum_event(0)
    sum_event(1)
    wait_cross(2, 6)
    weight_part([2, 6])
    tok_event(6)
    wait_cross(3, 5)
    weight_part([3, 5])
    wait_cross(4)
    weight_part([4], last_part=True)
    sc_a1[0]()
    sc_b1[0]()
    input_part(2)
    input_part(6)
    sum_event(2)
    input_part(1)
    sum_event(3)
    sc_a1[1]()
    sc_b1[1]()
    input_part(7)
    sum_event(4)
    input_part(0)
    sc_a1[2]()
    sc_b1[2]()
    for q in range(4):
        DA2[q] = sc_a1[3](q // 2, q % 2).astype(BF16).reshape(2, quarter, 128)
        DB2[q] = sc_b1[3](q // 2, q % 2).astype(BF16).reshape(2, quarter, 128)
    sc_a2[0]()
    sc_b2[0]()
    sum_event(5)
    sc_a2[1]()
    sc_b2[1]()
    sum_event(6)
    sc_a2[2]()
    sc_b2[2]()
    norms = []
    for scat, out in ((sc_a2, gwg_o), (sc_b2, vwg_o)):
        grad = scat[3]().reshape(WIDTH, 128)
        norms.append(jnp.sum(grad * grad, axis=0, keepdims=True))
        out[...] = grad
    NC[c, 0, 0:1] = norms[0]
    NC[c, 0, 1:2] = norms[1]
    pair = remote(NC.at[c], NC.at[c], c=p)
    pair.wait_recv()
    NZ[z] = NC[0] + NC[1]
    along = [remote(NZ.at[z], NZ.at[z], z=ahead(z, k, 8)) for k in range(1, 8)]
    partner[0].wait_recv()
    for d in range(2):
        flow[d, 5].wait_recv()
        flow[d, 6].wait_recv()

    for h in range(2):
        j_up = 6 if h == 0 else 5
        j_dn = 5 if h == 0 else 6

        def step(i, _, h=h, j_up=j_up, j_dn=j_dn):
            rows = pl.ds(pl.multiple_of(h * 64 + i * 16, 16), 16)
            here = pl.ds(pl.multiple_of(i * 16, 16), 16)
            v = PB[0, c, rows, :].astype(F32) + PX[0, rows, :].astype(F32)
            v = v + RS[0, j_up, here, :].astype(F32) + RS[1, j_dn, here, :].astype(F32)
            ig_o[rows, :] = v.astype(BF16)
            return 0

        lax.fori_loop(0, 4, step, 0)

    for copy in along:
        copy.wait_recv()
    total = NZ[0]
    for k in range(1, 8):
        total = total + NZ[k]
    gn_o[...] = total[0, 0:1]
    vn_o[...] = total[0, 1:2]
    diagonal = lax.broadcasted_iota(jnp.int32, (8, 128), 0) == lax.broadcasted_iota(
        jnp.int32, (8, 128), 1
    )
    for q in range(2):
        row = jnp.sum(jnp.where(diagonal, total[1 + q], 0.0), axis=0, keepdims=True)
        tn_o[q : q + 1, :] = row[:, 0:3]
    for copy in started:
        copy.wait_send()
    assert len(started) == N_COPIES, len(started)


def finish(*refs):
    for src, dst in zip(refs[:8], refs[8:]):
        dst[...] = src[...]


def local(tokens, up_gate, up_val, gate_weight, val_weight, gate_taps, val_taps, hidden_grad):
    hbm = pl.BlockSpec(memory_space=pl.ANY)
    vmem = pl.BlockSpec(memory_space=pltpu.VMEM)
    half = WIDTH // 2
    scratch = [
        pltpu.VMEM((8, 256, D), BF16),
        pltpu.VMEM((WIDTH, 2 * SEQ), BF16),
        pltpu.VMEM((WIDTH, 2 * SEQ), BF16),
        pltpu.VMEM((WIDTH, 2 * SEQ), BF16),
        pltpu.VMEM((2, WIDTH, 128), F32),
        pltpu.VMEM((2, WIDTH, 128), F32),
        pltpu.VMEM((2 * SEQ, BOTH), BF16),
        pltpu.VMEM((8, BOTH, 256), BF16),
        pltpu.VMEM((4, 4, BOTH, ROWS), BF16),
        pltpu.VMEM((8, BOTH, 256), F32),
        pltpu.VMEM((4, 2, 2, WIDTH, 128), BF16),
        pltpu.VMEM((4, 2, 2, WIDTH, 128), BF16),
        pltpu.VMEM((4, 2, half, 128), BF16),
        pltpu.VMEM((4, 2, half, 128), BF16),
        pltpu.VMEM((2, 2, WIDTH, 128), BF16),
        pltpu.VMEM((2, 2, 2, WIDTH, 128), BF16),
        pltpu.VMEM((2, 2, WIDTH, 128), BF16),
        pltpu.VMEM((2, 2, 2, WIDTH, 128), BF16),
        pltpu.VMEM((2, half, 128), BF16),
        pltpu.VMEM((2, 2, half, 128), BF16),
        pltpu.VMEM((2, half, 128), BF16),
        pltpu.VMEM((2, 2, half, 128), BF16),
        pltpu.VMEM((8, 2, ROWS, D), BF16),
        pltpu.VMEM((8, ROWS, D), BF16),
        pltpu.VMEM((2, 7, 64, D), BF16),
        pltpu.VMEM((4, 2, 8, WIDTH), F32),
        pltpu.VMEM((4, 2, 8, WIDTH), F32),
        pltpu.VMEM((2, 3, 8, 128), F32),
        pltpu.VMEM((8, 3, 8, 128), F32),
        pltpu.SemaphoreType.DMA((6,)),
        pltpu.SemaphoreType.DMA((N_COPIES,)),
        pltpu.SemaphoreType.DMA((N_COPIES,)),
    ]
    out = pl.pallas_call(
        kernel,
        out_shape=[
            jax.ShapeDtypeStruct((ROWS, D), BF16),
            jax.ShapeDtypeStruct((WIDTH, ROWS), F32),
            jax.ShapeDtypeStruct((WIDTH, ROWS), F32),
            jax.ShapeDtypeStruct((3, WIDTH), F32),
            jax.ShapeDtypeStruct((3, WIDTH), F32),
            jax.ShapeDtypeStruct((1, ROWS), F32),
            jax.ShapeDtypeStruct((1, ROWS), F32),
            jax.ShapeDtypeStruct((2, 3), F32),
        ],
        in_specs=[hbm, hbm, hbm, hbm, hbm, vmem, vmem, hbm],
        out_specs=[vmem] * 8,
        scratch_shapes=scratch,
        compiler_params=pltpu.CompilerParams(
            collective_id=0, has_side_effects=True, vmem_limit_bytes=67_000_000
        ),
        name="backward",
    )(tokens, up_gate.T, up_val.T, gate_weight.T, val_weight.T, gate_taps, val_taps, hidden_grad.T)
    out = pl.pallas_call(
        finish,
        out_shape=[jax.ShapeDtypeStruct(a.shape, a.dtype) for a in out],
        in_specs=[vmem] * 8,
        out_specs=[vmem] * 8,
        name="finish",
    )(*out)
    return (out[0], out[1].T, out[2].T, out[3], out[4], out[5].reshape(ROWS), out[6].reshape(ROWS), out[7])


def solution(mesh):
    split = Mesh(mesh.devices.reshape(4, 4, 8, 2), ("y", "x", "z", "c"))
    fs, tp, both = ("y", "x"), ("z", "c"), ("y", "x", "z", "c")
    in_specs = (
        P(both, None), P(fs, tp), P(fs, tp), P(fs, tp), P(fs, tp), P(None, tp), P(None, tp), P(fs, tp),
    )
    out_specs = (
        P(both, None), P(fs, tp), P(fs, tp), P(None, tp), P(None, tp), P(fs), P(fs), P(),
    )
    return jax.shard_map(local, mesh=split, in_specs=in_specs, out_specs=out_specs, check_vma=False)
```

```python
import itertools

import jax
import jax.numpy as jnp
from jax import lax
from jax.experimental import pallas as pl
from jax.experimental.pallas import tpu as pltpu
from jax.sharding import Mesh
from jax.sharding import PartitionSpec as P

F32, BF16 = jnp.float32, jnp.bfloat16
MESH = pl.DeviceIdType.MESH
SEQ = 1024
D = 2048
ROWS = 128
WIDTH = 352
BOTH = 2 * WIDTH
GROUP = 16
TILES = SEQ // 128
NN = (((1,), (0,)), ((), ()))
N_COPIES = 106


def kernel(
    tok, ug, uv, gw, vw, gt, vt, hg,
    own_o, cross_o, last_o, gwg_o, vwg_o, small_o,
    TOK, UGI, UVI, HGI, GT, VT, SM, GW, KT, TS, UB, UBT, W, ACC, DA, DB, DA2, DB2,
    RA0, RA1, RB0, RB1, SA0, SA1, SB0, SB1, PB, PX, RS, TX, TY, NC, NZ,
    lsem, ssem, rsem,
):
    y, x, z, c = (lax.axis_index(a) for a in ("y", "x", "z", "c"))
    p = 1 - c

    def ahead(i, k, n):
        return lax.rem(i + k, n)

    ids = itertools.count()
    started = []

    def remote(src, dst, **dev):
        i = next(ids)
        copy = pltpu.make_async_remote_copy(
            src_ref=src, dst_ref=dst, send_sem=ssem.at[i], recv_sem=rsem.at[i],
            device_id=dev, device_id_type=MESH,
        )
        copy.start()
        started.append(copy)
        return copy

    def load(src, dst, i):
        copy = pltpu.make_async_copy(src, dst, lsem.at[i])
        copy.start()
        return copy

    own_rows = pl.ds(pl.multiple_of(c * ROWS, ROWS), ROWS)
    l_tok = load(tok, TOK.at[z, own_rows], 0)
    l_gw = load(gw, W.at[y, x, pl.ds(0, WIDTH)], 1)
    l_vw = load(vw, W.at[y, x, pl.ds(WIDTH, WIDTH)], 2)
    pairs = (gt, GT), (vt, VT), (ug, UGI), (uv, UVI), (hg, HGI)
    l_in = [load(a, b, 3 + i) for i, (a, b) in enumerate(pairs)]

    barrier = pltpu.get_barrier_semaphore()
    peers = [{"c": p}]
    peers += [{"x": ahead(x, k, 4)} for k in (1, 2, 3)]
    peers += [{"y": ahead(y, k, 4)} for k in (1, 2, 3)]
    peers += [{"z": ahead(z, k, 8)} for k in range(1, 8)]
    for peer in peers:
        pl.semaphore_signal(barrier, inc=1, device_id=peer, device_id_type=MESH)

    l_tok.wait()
    pl.semaphore_wait(barrier, len(peers))

    def tok_at(zz, core, h):
        return TOK.at[zz, pl.ds(pl.multiple_of(core * ROWS + h * 64, 64), 64)]

    order_up = [(0, 0), (0, 1), (1, 0), (1, 1), (2, 0), (2, 1), (3, 0)]
    order_dn = [(s, 1 - h) for s, h in order_up]
    up, down, cross = {}, {}, {}

    def tok_send(j):
        s, h = order_up[j]
        blk = tok_at(ahead(z, 8 - s, 8), c, h)
        up[j] = remote(blk, blk, z=ahead(z, 1, 8))
        s, h = order_dn[j]
        blk = tok_at(ahead(z, s, 8), c, h)
        down[j] = remote(blk, blk, z=ahead(z, 7, 8))

    def tok_cross(k, h):
        blk = tok_at(ahead(z, k, 8), c, h)
        cross[k, h] = remote(blk, blk, c=p)

    def tok_event(j):
        up[j].wait_recv()
        down[j].wait_recv()
        if j + 2 < 7:
            tok_send(j + 2)
        s, h = order_up[j]
        tok_cross(7 - s, h)
        s, h = order_dn[j]
        tok_cross(1 + s, h)

    tok_send(0)
    tok_send(1)
    tok_cross(0, 0)
    tok_cross(0, 1)

    def gather(slot, axis, i):
        state = {}

        def begin():
            for d, s in ((0, 1), (1, 3)):
                state[d] = remote(slot(i, None), slot(i, None), **{axis: ahead(i, s, 4)})

        def middle():
            for d, s in ((0, 1), (1, 3)):
                state[d].wait_recv()
                far = ahead(i, 4 - s, 4)
                state[2 + d] = remote(slot(far, d), slot(far, d), **{axis: ahead(i, s, 4)})

        def end():
            state[2].wait_recv()
            state[3].wait_recv()

        return begin, middle, end

    quarter = WIDTH // 2

    def a1(i, d):
        return W.at[y, i, pl.ds(0, WIDTH) if d is None else pl.ds(quarter * d, quarter)]

    def b1(i, d):
        rows = pl.ds(WIDTH, WIDTH) if d is None else pl.ds(WIDTH + quarter * d, quarter)
        return W.at[i, x, rows]

    def a2(i, d):
        return W.at[i, pl.ds(0, 4) if d is None else pl.ds(2 * d, 2), pl.ds(0, WIDTH)]

    def b2(i, d):
        return W.at[pl.ds(0, 4) if d is None else pl.ds(2 * d, 2), i, pl.ds(WIDTH, WIDTH)]

    first = gather(a1, "x", x), gather(b1, "y", y)
    second = gather(a2, "y", y), gather(b2, "x", x)
    l_gw.wait()
    l_vw.wait()
    for g in first:
        g[0]()

    for copy in l_in:
        copy.wait()
    for q, ref in enumerate((GT, VT)):
        rows = jnp.concatenate([ref[...].astype(F32), jnp.zeros((5, WIDTH), F32)], axis=0)
        for t in range(3):
            lo, hi = t * 128, min(t * 128 + 128, WIDTH)
            KT[q, lo:hi, 0:8] = rows[:, lo:hi].T

    lane = lax.broadcasted_iota(jnp.int32, (GROUP, 128), 1)
    edge = {1: lane >= 1, 2: lane >= 2, -1: lane < 127, -2: lane < 126}
    nil = jnp.zeros((GROUP, 128), F32)

    def moved(tiles, k):
        turned = [pltpu.roll(a, k % 128, 1) for a in tiles]
        if k > 0:
            other = [nil] + turned[:-1]
        else:
            other = turned[1:] + [nil]
        return [jnp.where(edge[k], a, b) for a, b in zip(turned, other)]

    def conv(first_group, last_group):
        def step(g, _):
            rows = pl.ds(pl.multiple_of(g * GROUP, GROUP), GROUP)
            low = pl.ds(pl.multiple_of(WIDTH + g * GROUP, GROUP), GROUP)
            kg = [jnp.broadcast_to(KT[0, rows, i : i + 1], (GROUP, 128)) for i in range(3)]
            kv = [jnp.broadcast_to(KT[1, rows, i : i + 1], (GROUP, 128)) for i in range(3)]
            sums = [nil] * 6
            for s in range(2):
                at = [slice(s * SEQ + i * 128, s * SEQ + i * 128 + 128) for i in range(TILES)]
                g0 = [UGI[rows, a].astype(F32) for a in at]
                v0 = [UVI[rows, a].astype(F32) for a in at]
                g1, g2, v1, v2 = moved(g0, 1), moved(g0, 2), moved(v0, 1), moved(v0, 2)
                gb, vb = [], []
                for i in range(TILES):
                    h = HGI[rows, at[i]].astype(F32)
                    cg = kg[0] * g2[i] + kg[1] * g1[i] + kg[2] * g0[i]
                    cv = kv[0] * v2[i] + kv[1] * v1[i] + kv[2] * v0[i]
                    sg = jax.nn.sigmoid(cg)
                    hs = h * sg
                    vb.append(hs * cg)
                    gb.append(hs * cv * (1.0 + cg * (1.0 - sg)))
                    terms = [u * gb[i] for u in (g2[i], g1[i], g0[i])]
                    terms += [u * vb[i] for u in (v2[i], v1[i], v0[i])]
                    sums = [a + b for a, b in zip(sums, terms)]
                gb1, gb2, vb1, vb2 = moved(gb, -1), moved(gb, -2), moved(vb, -1), moved(vb, -2)
                for i in range(TILES):
                    half = slice((i % 2) * 128, (i % 2) * 128 + 128)
                    og = kg[2] * gb[i] + kg[1] * gb1[i] + kg[0] * gb2[i]
                    ov = kv[2] * vb[i] + kv[1] * vb1[i] + kv[0] * vb2[i]
                    UBT[4 * s + i // 2, rows, half] = og.astype(BF16)
                    UBT[4 * s + i // 2, low, half] = ov.astype(BF16)
            for q in range(2):
                t = [jnp.sum(sums[3 * q + i], axis=1, keepdims=True) for i in range(3)]
                TS[q, rows, :] = jnp.where(
                    lane == 0, t[0], jnp.where(lane == 1, t[1], jnp.where(lane == 2, t[2], 0.0))
                )
            return 0

        lax.fori_loop(first_group, last_group, step, 0)

    def turn(zz):
        rows = pl.ds(pl.multiple_of(zz * 256, 256), 256)
        for lo in range(0, BOTH, 128):
            hi = min(lo + 128, BOTH)
            UB[rows, lo:hi] = UBT[zz, lo:hi, :].T

    def weight_part(ks, first_part=False, last_part=False):
        zs = [ahead(z, k, 8) for k in ks]

        def step(n, _):
            cols = pl.ds(pl.multiple_of(n * 256, 256), 256)
            total = None
            for zz in zs:
                part = lax.dot_general(UBT[zz], TOK[zz, :, cols], NN, preferred_element_type=F32)
                total = part if total is None else total + part
            if not first_part:
                total = total + ACC[n]
            if last_part:
                out = total.astype(BF16)
                yy, xx = n // 2, 2 * (n % 2)
                for q in range(2):
                    DA[xx + q, yy // 2, yy % 2] = out[0:WIDTH, q * 128 : q * 128 + 128]
                    DB[yy, xx // 2, q] = out[WIDTH:BOTH, q * 128 : q * 128 + 128]
            else:
                ACC[n] = total
            return 0

        lax.fori_loop(0, 8, step, 0)

    def wait_cross(*ks):
        for k in ks:
            cross[k, 0].wait_recv()
            cross[k, 1].wait_recv()

    partner = {}

    def input_part(k):
        zz = ahead(z, k, 8)
        rows = pl.ds(pl.multiple_of(zz * 256, 256), 256)

        def step(n, _):
            yy, xx = n // 2, 2 * (n % 2)
            w = jnp.concatenate([W[yy, xx], W[yy, xx + 1]], axis=1)
            out = lax.dot_general(UB[rows, :], w, NN, preferred_element_type=F32).astype(BF16)
            cols = pl.ds(pl.multiple_of(n * 256, 256), 256)
            PB[k, 0, :, cols] = out[0:128]
            PB[k, 1, :, cols] = out[128:256]
            return 0

        lax.fori_loop(0, 8, step, 0)
        partner[k] = remote(PB.at[k, p], PX.at[k] if k else cross_o, c=p)

    sum_up = [(0, 0), (1, 1), (1, 0), (2, 1), (2, 0), (3, 1), (3, 0)]
    flow = {}

    def pair_sum(k, h, extra):
        def step(i, _):
            rows = pl.ds(pl.multiple_of(h * 64 + i * 16, 16), 16)
            v = PB[k, c, rows, :].astype(F32) + PX[k, rows, :].astype(F32)
            if extra is not None:
                v = v + RS[extra[0], extra[1], pl.ds(pl.multiple_of(i * 16, 16), 16), :].astype(F32)
            PB[k, c, rows, :] = v.astype(BF16)
            return 0

        lax.fori_loop(0, 4, step, 0)

    def sum_event(j):
        for d in range(2):
            s, h = sum_up[j]
            if d:
                h = 1 - h
            k = 4 - s if d == 0 else 4 + s
            if j == 0 and d == 0 or j == 1 or j == 3 or j == 5:
                partner[k].wait_recv()
            if j >= 2:
                flow[d, j - 2].wait_recv()
            pair_sum(k, h, (d, j - 2) if j >= 2 else None)
            flow[d, j] = remote(
                PB.at[k, c, pl.ds(h * 64, 64)],
                RS.at[d, j] if s < 3 else last_o.at[d, pl.ds(h * 64, 64)],
                z=ahead(z, 1 if d == 0 else 7, 8),
            )

    def scatter(src, r0, r1, axis, i):
        state = {}
        own = i
        near = {0: ahead(i, 1, 4), 1: ahead(i, 3, 4)}
        far = ahead(i, 2, 4)

        def begin():
            for d in range(2):
                to = {axis: near[d]}
                state[d] = remote(src.at[far, d], r0.at[d], **to)
                state[2 + d] = remote(src.at[near[d], 1 - d], r1.at[d, 1 - d], **to)

        def middle():
            for d in range(2):
                state[d].wait_recv()
                src[near[d], d] = (src[near[d], d].astype(F32) + r0[d].astype(F32)).astype(BF16)
                state[4 + d] = remote(src.at[near[d], d], r1.at[d, d], **{axis: near[d]})

        def end():
            for i_ in range(2, 6):
                state[i_].wait_recv()

        def total(*at):
            t = src[(own, *at)].astype(F32)
            return t + r1[(0, *at)].astype(F32) + r1[(1, *at)].astype(F32)

        return begin, middle, end, total

    sc_a1 = scatter(DA, RA0, RA1, "x", x)
    sc_b1 = scatter(DB, RB0, RB1, "y", y)
    sc_a2 = scatter(DA2, SA0, SA1, "y", y)
    sc_b2 = scatter(DB2, SB0, SB1, "x", x)

    def tap_sum(ref):
        return ref[0] + ref[1] + ref[2] + ref[3]

    conv(0, 8)
    for g in first:
        g[1]()
    conv(8, 15)
    tok_event(0)
    for g in first:
        g[2]()
    for g in second:
        g[0]()
    conv(15, 22)
    for q in range(2):
        for lo in range(0, WIDTH, 128):
            hi = min(lo + 128, WIDTH)
            TX[x, q, :, lo:hi] = TS[q, lo:hi, :].T[0:8]
    tap_x = [remote(TX.at[x], TX.at[x], x=ahead(x, k, 4)) for k in (1, 2, 3)]
    lax.fori_loop(0, 8, lambda i, _: (turn(i), 0)[1], 0)
    tok_event(1)
    wait_cross(0)
    weight_part([0], first_part=True)
    wait_cross(1, 7)
    weight_part([1, 7])
    for g in second:
        g[1]()
    tok_event(2)
    for copy in tap_x:
        copy.wait_recv()
    TY[y] = tap_sum(TX)
    tap_y = [remote(TY.at[y], TY.at[y], y=ahead(y, k, 4)) for k in (1, 2, 3)]
    tok_event(3)
    for g in second:
        g[2]()
    input_part(4)
    input_part(3)
    tok_event(4)
    input_part(5)
    sum_event(0)
    sum_event(1)
    wait_cross(2, 6)
    weight_part([2, 6])
    tok_event(5)
    input_part(2)
    wait_cross(3, 5)
    weight_part([3, 5])
    tok_event(6)
    wait_cross(4)
    weight_part([4], last_part=True)
    sc_a1[0]()
    sc_b1[0]()
    input_part(6)
    sum_event(2)
    input_part(1)
    input_part(7)
    sc_a1[1]()
    sc_b1[1]()
    sum_event(3)
    input_part(0)
    own = load(PB.at[0, c], own_o, 0)
    for copy in tap_y:
        copy.wait_recv()
    taps = tap_sum(TY)
    for q in range(2):
        SM[8 * q : 8 * q + 8, :] = taps[q]
        square = jnp.sum(taps[q] * taps[q], axis=1, keepdims=True)
        NC[c, 1 + q] = jnp.broadcast_to(square, (8, 128))
    sum_event(4)
    sc_a1[2]()
    sc_b1[2]()
    for q in range(4):
        DA2[q] = sc_a1[3](q // 2, q % 2).astype(BF16).reshape(2, quarter, 128)
        DB2[q] = sc_b1[3](q // 2, q % 2).astype(BF16).reshape(2, quarter, 128)
    sc_a2[0]()
    sc_b2[0]()
    sc_a2[1]()
    sc_b2[1]()
    sum_event(5)
    sc_a2[2]()
    sc_b2[2]()
    NC[c, 0] = jnp.zeros((8, 128), F32)
    for q, scat in enumerate((sc_a2, sc_b2)):
        grad = scat[3]().reshape(WIDTH, 128)
        NC[c, 0, q : q + 1] = jnp.sum(grad * grad, axis=0, keepdims=True)
        GW[q] = grad
    pair = remote(NC.at[c], NC.at[c], c=p)
    results = [load(GW.at[0], gwg_o, 1), load(GW.at[1], vwg_o, 2)]
    pair.wait_recv()
    NZ[z] = NC[0] + NC[1]
    along = [remote(NZ.at[z], NZ.at[z], z=ahead(z, k, 8)) for k in range(1, 8)]
    sum_event(6)
    for copy in along:
        copy.wait_recv()
    total = NZ[0]
    for k in range(1, 8):
        total = total + NZ[k]
    diagonal = lax.broadcasted_iota(jnp.int32, (8, 128), 0) == lax.broadcasted_iota(
        jnp.int32, (8, 128), 1
    )
    SM[16:24, 0:128] = total[0]
    for q in range(2):
        row = jnp.sum(jnp.where(diagonal, total[1 + q], 0.0), axis=0, keepdims=True)
        SM[18 + q : 19 + q, 0:128] = row
    small = load(SM, small_o, 3)
    for copy in (own, *results, small):
        copy.wait()
    partner[0].wait_recv()
    for d in range(2):
        flow[d, 5].wait_recv()
        flow[d, 6].wait_recv()
    for copy in started:
        copy.wait_send()
    assert len(started) == N_COPIES, len(started)


def finish(own, cross, last, gwg, vwg, small, ig_o, gwg_o, vwg_o, gtg_o, vtg_o, gn_o, vn_o, tn_o):
    gwg_o[...] = gwg[...]
    vwg_o[...] = vwg[...]
    gtg_o[...] = small[0:3, :]
    vtg_o[...] = small[8:11, :]
    gn_o[...] = small[16:17, 0:128]
    vn_o[...] = small[17:18, 0:128]
    tn_o[...] = small[18:20, 0:3]
    value = own[...].astype(F32) + cross[...].astype(F32)
    ig_o[...] = (value + last[0].astype(F32) + last[1].astype(F32)).astype(BF16)


def local(tokens, up_gate, up_val, gate_weight, val_weight, gate_taps, val_taps, hidden_grad):
    hbm = pl.BlockSpec(memory_space=pl.ANY)
    vmem = pl.BlockSpec(memory_space=pltpu.VMEM)
    half = WIDTH // 2
    scratch = [
        pltpu.VMEM((8, 256, D), BF16),
        pltpu.VMEM((WIDTH, 2 * SEQ), BF16),
        pltpu.VMEM((WIDTH, 2 * SEQ), BF16),
        pltpu.VMEM((WIDTH, 2 * SEQ), BF16),
        pltpu.VMEM((3, WIDTH), BF16),
        pltpu.VMEM((3, WIDTH), BF16),
        pltpu.VMEM((24, WIDTH), F32),
        pltpu.VMEM((2, WIDTH, ROWS), F32),
        pltpu.VMEM((2, WIDTH, 128), F32),
        pltpu.VMEM((2, WIDTH, 128), F32),
        pltpu.VMEM((2 * SEQ, BOTH), BF16),
        pltpu.VMEM((8, BOTH, 256), BF16),
        pltpu.VMEM((4, 4, BOTH, ROWS), BF16),
        pltpu.VMEM((8, BOTH, 256), F32),
        pltpu.VMEM((4, 2, 2, WIDTH, 128), BF16),
        pltpu.VMEM((4, 2, 2, WIDTH, 128), BF16),
        pltpu.VMEM((4, 2, half, 128), BF16),
        pltpu.VMEM((4, 2, half, 128), BF16),
        pltpu.VMEM((2, 2, WIDTH, 128), BF16),
        pltpu.VMEM((2, 2, 2, WIDTH, 128), BF16),
        pltpu.VMEM((2, 2, WIDTH, 128), BF16),
        pltpu.VMEM((2, 2, 2, WIDTH, 128), BF16),
        pltpu.VMEM((2, half, 128), BF16),
        pltpu.VMEM((2, 2, half, 128), BF16),
        pltpu.VMEM((2, half, 128), BF16),
        pltpu.VMEM((2, 2, half, 128), BF16),
        pltpu.VMEM((8, 2, ROWS, D), BF16),
        pltpu.VMEM((8, ROWS, D), BF16),
        pltpu.VMEM((2, 7, 64, D), BF16),
        pltpu.VMEM((4, 2, 8, WIDTH), F32),
        pltpu.VMEM((4, 2, 8, WIDTH), F32),
        pltpu.VMEM((2, 3, 8, 128), F32),
        pltpu.VMEM((8, 3, 8, 128), F32),
        pltpu.SemaphoreType.DMA((8,)),
        pltpu.SemaphoreType.DMA((N_COPIES,)),
        pltpu.SemaphoreType.DMA((N_COPIES,)),
    ]
    out = pl.pallas_call(
        kernel,
        out_shape=[
            jax.ShapeDtypeStruct((ROWS, D), BF16),
            jax.ShapeDtypeStruct((ROWS, D), BF16),
            jax.ShapeDtypeStruct((2, ROWS, D), BF16),
            jax.ShapeDtypeStruct((WIDTH, ROWS), F32),
            jax.ShapeDtypeStruct((WIDTH, ROWS), F32),
            jax.ShapeDtypeStruct((24, WIDTH), F32),
        ],
        in_specs=[hbm] * 8,
        out_specs=[hbm] * 6,
        scratch_shapes=scratch,
        compiler_params=pltpu.CompilerParams(
            collective_id=0, has_side_effects=True, vmem_limit_bytes=67_000_000
        ),
        name="backward",
    )(tokens, up_gate.T, up_val.T, gate_weight.T, val_weight.T, gate_taps, val_taps, hidden_grad.T)
    out = pl.pallas_call(
        finish,
        out_shape=[
            jax.ShapeDtypeStruct((ROWS, D), BF16),
            jax.ShapeDtypeStruct((WIDTH, ROWS), F32),
            jax.ShapeDtypeStruct((WIDTH, ROWS), F32),
            jax.ShapeDtypeStruct((3, WIDTH), F32),
            jax.ShapeDtypeStruct((3, WIDTH), F32),
            jax.ShapeDtypeStruct((1, ROWS), F32),
            jax.ShapeDtypeStruct((1, ROWS), F32),
            jax.ShapeDtypeStruct((2, 3), F32),
        ],
        in_specs=[vmem] * 6,
        out_specs=[vmem] * 8,
        name="finish",
    )(*out)
    return (out[0], out[1].T, out[2].T, out[3], out[4], out[5].reshape(ROWS), out[6].reshape(ROWS), out[7])


def solution(mesh):
    split = Mesh(mesh.devices.reshape(4, 4, 8, 2), ("y", "x", "z", "c"))
    fs, tp, both = ("y", "x"), ("z", "c"), ("y", "x", "z", "c")
    in_specs = (
        P(both, None), P(fs, tp), P(fs, tp), P(fs, tp), P(fs, tp), P(None, tp), P(None, tp), P(fs, tp),
    )
    out_specs = (
        P(both, None), P(fs, tp), P(fs, tp), P(None, tp), P(None, tp), P(fs), P(fs), P(),
    )
    return jax.shard_map(local, mesh=split, in_specs=in_specs, out_specs=out_specs, check_vma=False)
```

```python
import itertools

import jax
import jax.numpy as jnp
from jax import lax
from jax.experimental import pallas as pl
from jax.experimental.pallas import tpu as pltpu
from jax.sharding import Mesh
from jax.sharding import PartitionSpec as P

F32, BF16 = jnp.float32, jnp.bfloat16
MESH = pl.DeviceIdType.MESH
SEQ = 1024
D = 2048
ROWS = 128
WIDTH = 352
BOTH = 2 * WIDTH
GROUP = 16
TILES = SEQ // 128
NN = (((1,), (0,)), ((), ()))
N_RECV, N_SEND = 50, 14


def kernel(
    tok, ug, uv, gw, vw, gt, vt, hg,
    base_o, last_o, gwg_o, vwg_o, small_o,
    TOK, UGI, UVI, HGI, GT, VT, SM, GW, KT, TS, UB, UBT, W, ACC, DA, DB, DA2, DB2,
    RA0, RA1, RB0, RB1, SA0, SA1, SB0, SB1, PB, PX, RS, TX, TY, NC, NZ, BASE,
    lsem, send_sem, recv_sem,
):
    y, x, z, c = (lax.axis_index(a) for a in ("y", "x", "z", "c"))
    p = 1 - c

    def ahead(i, k, n):
        return lax.rem(i + k, n)

    recv_ids, send_ids = itertools.count(), itertools.count()
    sent = []

    class Group:
        def __init__(self, carrier):
            self.carrier = carrier
            self.sem = recv_sem.at[next(recv_ids)]

        def wait(self):
            pltpu.make_async_copy(self.carrier, self.carrier, self.sem).wait()

    def family(carrier):
        sem = send_sem.at[next(send_ids)]
        sent.append((carrier, sem))

        def remote(group, src, dst, **dev):
            pltpu.make_async_remote_copy(
                src_ref=src, dst_ref=dst, send_sem=sem, recv_sem=group.sem,
                device_id=dev, device_id_type=MESH,
            ).start()

        return remote

    def load(src, dst, i):
        copy = pltpu.make_async_copy(src, dst, lsem.at[i])
        copy.start()
        return copy

    own_rows = pl.ds(pl.multiple_of(c * ROWS, ROWS), ROWS)
    l_tok = load(tok, TOK.at[z, own_rows], 0)
    l_gw = load(gw, W.at[y, x, pl.ds(0, WIDTH)], 1)
    l_vw = load(vw, W.at[y, x, pl.ds(WIDTH, WIDTH)], 2)
    pairs = (gt, GT), (vt, VT), (ug, UGI), (uv, UVI), (hg, HGI)
    l_in = [load(a, b, 3 + i) for i, (a, b) in enumerate(pairs)]

    barrier = pltpu.get_barrier_semaphore()
    peers = [{"c": p}]
    peers += [{"x": ahead(x, k, 4)} for k in (1, 2, 3)]
    peers += [{"y": ahead(y, k, 4)} for k in (1, 2, 3)]
    peers += [{"z": ahead(z, k, 8)} for k in range(1, 8)]
    for peer in peers:
        pl.semaphore_signal(barrier, inc=1, device_id=peer, device_id_type=MESH)

    l_tok.wait()
    pl.semaphore_wait(barrier, len(peers))

    def tok_at(zz, core, h):
        return TOK.at[zz, pl.ds(pl.multiple_of(core * ROWS + h * 64, 64), 64)]

    order_up = [(0, 0), (0, 1), (1, 0), (1, 1), (2, 0), (2, 1), (3, 0)]
    order_dn = [(s, 1 - h) for s, h in order_up]
    around, cross = {}, {}
    send_tok, send_cross = family(RS), family(TOK.at[pl.ds(0, 4)])

    def tok_send(j):
        around[j] = Group(TOK.at[0, pl.ds(0, 128)])
        s, h = order_up[j]
        blk = tok_at(ahead(z, 8 - s, 8), c, h)
        send_tok(around[j], blk, blk, z=ahead(z, 1, 8))
        s, h = order_dn[j]
        blk = tok_at(ahead(z, s, 8), c, h)
        send_tok(around[j], blk, blk, z=ahead(z, 7, 8))

    def tok_cross(k, h):
        if k not in cross:
            cross[k] = Group(TOK.at[0, pl.ds(0, 128)])
        blk = tok_at(ahead(z, k, 8), c, h)
        send_cross(cross[k], blk, blk, c=p)

    def tok_event(j):
        around[j].wait()
        if j + 2 < 7:
            tok_send(j + 2)
        s, h = order_up[j]
        tok_cross(7 - s, h)
        s, h = order_dn[j]
        tok_cross(1 + s, h)

    tok_send(0)
    tok_send(1)
    tok_cross(0, 0)
    tok_cross(0, 1)

    def gather(remote, slot, axis, i, near_bytes, far_bytes):
        near, far = Group(near_bytes), Group(far_bytes)

        def begin():
            for s in (1, 3):
                remote(near, slot(i, None), slot(i, None), **{axis: ahead(i, s, 4)})

        def middle():
            near.wait()
            for d, s in ((0, 1), (1, 3)):
                blk = slot(ahead(i, 4 - s, 4), d)
                remote(far, blk, blk, **{axis: ahead(i, s, 4)})

        return begin, middle, far.wait

    quarter = WIDTH // 2

    def a1(i, d):
        return W.at[y, i, pl.ds(0, WIDTH) if d is None else pl.ds(quarter * d, quarter)]

    def b1(i, d):
        rows = pl.ds(WIDTH, WIDTH) if d is None else pl.ds(WIDTH + quarter * d, quarter)
        return W.at[i, x, rows]

    def a2(i, d):
        return W.at[i, pl.ds(0, 4) if d is None else pl.ds(2 * d, 2), pl.ds(0, WIDTH)]

    def b2(i, d):
        return W.at[pl.ds(0, 4) if d is None else pl.ds(2 * d, 2), i, pl.ds(WIDTH, WIDTH)]

    send_first, send_second = family(W.at[0, pl.ds(0, 3)]), family(W.at[pl.ds(0, 3)])
    near1, far1 = W.at[0, 0], W.at[0, 0, pl.ds(0, WIDTH)]
    near2, far2 = W.at[0], W.at[0, pl.ds(0, 2)]
    first = (
        gather(send_first, a1, "x", x, near1, far1),
        gather(send_first, b1, "y", y, near1, far1),
    )
    second = (
        gather(send_second, a2, "y", y, near2, far2),
        gather(send_second, b2, "x", x, near2, far2),
    )
    l_gw.wait()
    l_vw.wait()
    for g in first:
        g[0]()

    for copy in l_in:
        copy.wait()
    for q, ref in enumerate((GT, VT)):
        rows = jnp.concatenate([ref[...].astype(F32), jnp.zeros((5, WIDTH), F32)], axis=0)
        for t in range(3):
            lo, hi = t * 128, min(t * 128 + 128, WIDTH)
            KT[q, lo:hi, 0:8] = rows[:, lo:hi].T

    lane = lax.broadcasted_iota(jnp.int32, (GROUP, 128), 1)
    edge = {1: lane >= 1, 2: lane >= 2, -1: lane < 127, -2: lane < 126}
    nil = jnp.zeros((GROUP, 128), F32)

    def moved(tiles, k):
        turned = [pltpu.roll(a, k % 128, 1) for a in tiles]
        if k > 0:
            other = [nil] + turned[:-1]
        else:
            other = turned[1:] + [nil]
        return [jnp.where(edge[k], a, b) for a, b in zip(turned, other)]

    def conv(first_group, last_group):
        def step(g, _):
            rows = pl.ds(pl.multiple_of(g * GROUP, GROUP), GROUP)
            low = pl.ds(pl.multiple_of(WIDTH + g * GROUP, GROUP), GROUP)
            kg = [jnp.broadcast_to(KT[0, rows, i : i + 1], (GROUP, 128)) for i in range(3)]
            kv = [jnp.broadcast_to(KT[1, rows, i : i + 1], (GROUP, 128)) for i in range(3)]
            sums = [nil] * 6
            for s in range(2):
                at = [slice(s * SEQ + i * 128, s * SEQ + i * 128 + 128) for i in range(TILES)]
                g0 = [UGI[rows, a].astype(F32) for a in at]
                v0 = [UVI[rows, a].astype(F32) for a in at]
                g1, g2, v1, v2 = moved(g0, 1), moved(g0, 2), moved(v0, 1), moved(v0, 2)
                gb, vb = [], []
                for i in range(TILES):
                    h = HGI[rows, at[i]].astype(F32)
                    cg = kg[0] * g2[i] + kg[1] * g1[i] + kg[2] * g0[i]
                    cv = kv[0] * v2[i] + kv[1] * v1[i] + kv[2] * v0[i]
                    sg = jax.nn.sigmoid(cg)
                    hs = h * sg
                    vb.append(hs * cg)
                    gb.append(hs * cv * (1.0 + cg * (1.0 - sg)))
                    terms = [u * gb[i] for u in (g2[i], g1[i], g0[i])]
                    terms += [u * vb[i] for u in (v2[i], v1[i], v0[i])]
                    sums = [a + b for a, b in zip(sums, terms)]
                gb1, gb2, vb1, vb2 = moved(gb, -1), moved(gb, -2), moved(vb, -1), moved(vb, -2)
                for i in range(TILES):
                    half = slice((i % 2) * 128, (i % 2) * 128 + 128)
                    og = kg[2] * gb[i] + kg[1] * gb1[i] + kg[0] * gb2[i]
                    ov = kv[2] * vb[i] + kv[1] * vb1[i] + kv[0] * vb2[i]
                    UBT[4 * s + i // 2, rows, half] = og.astype(BF16)
                    UBT[4 * s + i // 2, low, half] = ov.astype(BF16)
            for q in range(2):
                t = [jnp.sum(sums[3 * q + i], axis=1, keepdims=True) for i in range(3)]
                TS[q, rows, :] = jnp.where(
                    lane == 0, t[0], jnp.where(lane == 1, t[1], jnp.where(lane == 2, t[2], 0.0))
                )
            return 0

        lax.fori_loop(first_group, last_group, step, 0)

    def turn(zz):
        rows = pl.ds(pl.multiple_of(zz * 256, 256), 256)
        for lo in range(0, BOTH, 128):
            hi = min(lo + 128, BOTH)
            UB[rows, lo:hi] = UBT[zz, lo:hi, :].T

    def weight_part(ks, first_part=False, last_part=False):
        zs = [ahead(z, k, 8) for k in ks]

        def step(n, _):
            cols = pl.ds(pl.multiple_of(n * 256, 256), 256)
            total = None
            for zz in zs:
                part = lax.dot_general(UBT[zz], TOK[zz, :, cols], NN, preferred_element_type=F32)
                total = part if total is None else total + part
            if not first_part:
                total = total + ACC[n]
            if last_part:
                out = total.astype(BF16)
                yy, xx = n // 2, 2 * (n % 2)
                for q in range(2):
                    DA[xx + q, yy // 2, yy % 2] = out[0:WIDTH, q * 128 : q * 128 + 128]
                    DB[yy, xx // 2, q] = out[WIDTH:BOTH, q * 128 : q * 128 + 128]
            else:
                ACC[n] = total
            return 0

        lax.fori_loop(0, 8, step, 0)

    def wait_cross(*ks):
        for k in ks:
            cross[k].wait()

    partner = {}
    send_part = family(PX)

    def input_part(k):
        zz = ahead(z, k, 8)
        rows = pl.ds(pl.multiple_of(zz * 256, 256), 256)

        def step(n, _):
            yy, xx = n // 2, 2 * (n % 2)
            w = jnp.concatenate([W[yy, xx], W[yy, xx + 1]], axis=1)
            out = lax.dot_general(UB[rows, :], w, NN, preferred_element_type=F32).astype(BF16)
            cols = pl.ds(pl.multiple_of(n * 256, 256), 256)
            PB[k, 0, :, cols] = out[0:128]
            PB[k, 1, :, cols] = out[128:256]
            return 0

        lax.fori_loop(0, 8, step, 0)
        partner[k] = Group(PX.at[0])
        send_part(partner[k], PB.at[k, p], PX.at[k], c=p)

    sum_up = [(0, 0), (1, 1), (1, 0), (2, 1), (2, 0), (3, 1), (3, 0)]
    flow = {}
    send_flow = family(RS)

    def pair_sum(k, h, extra, dst=None):
        def step(i, _):
            rows = pl.ds(pl.multiple_of(h * 64 + i * 16, 16), 16)
            v = PB[k, c, rows, :].astype(F32) + PX[k, rows, :].astype(F32)
            if extra is not None:
                v = v + RS[extra[0], extra[1], pl.ds(pl.multiple_of(i * 16, 16), 16), :].astype(F32)
            if dst is None:
                PB[k, c, rows, :] = v.astype(BF16)
            else:
                dst[rows, :] = v.astype(BF16)
            return 0

        lax.fori_loop(0, 4, step, 0)

    def sum_event(j):
        s = sum_up[j][0]
        ks = (4 - s, 4 + s)
        if j in (0, 1, 3, 5):
            for k in sorted(set(ks)):
                partner[k].wait()
        if j >= 2:
            flow[j - 2].wait()
        flow[j] = Group(TOK.at[0, pl.ds(0, 128)])
        for d in range(2):
            h = sum_up[j][1] if d == 0 else 1 - sum_up[j][1]
            pair_sum(ks[d], h, (d, j - 2) if j >= 2 else None)
            send_flow(
                flow[j],
                PB.at[ks[d], c, pl.ds(h * 64, 64)],
                RS.at[d, j] if j < 6 else last_o.at[pl.ds(h * 64, 64)],
                z=ahead(z, 1 if d == 0 else 7, 8),
            )

    def scatter(src, r0, r1, axis, i):
        own = i
        near = {0: ahead(i, 1, 4), 1: ahead(i, 3, 4)}
        far = ahead(i, 2, 4)
        remote = family(src.at[pl.ds(0, 3)])
        early, late = Group(r0), Group(r1)

        def begin():
            for d in range(2):
                to = {axis: near[d]}
                remote(early, src.at[far, d], r0.at[d], **to)
                remote(late, src.at[near[d], 1 - d], r1.at[d, 1 - d], **to)

        def middle():
            early.wait()
            for d in range(2):
                src[near[d], d] = (src[near[d], d].astype(F32) + r0[d].astype(F32)).astype(BF16)
                remote(late, src.at[near[d], d], r1.at[d, d], **{axis: near[d]})

        end = late.wait

        def total(*at):
            t = src[(own, *at)].astype(F32)
            return t + r1[(0, *at)].astype(F32) + r1[(1, *at)].astype(F32)

        return begin, middle, end, total

    sc_a1 = scatter(DA, RA0, RA1, "x", x)
    sc_b1 = scatter(DB, RB0, RB1, "y", y)
    sc_a2 = scatter(DA2, SA0, SA1, "y", y)
    sc_b2 = scatter(DB2, SB0, SB1, "x", x)

    def tap_sum(ref):
        return ref[0] + ref[1] + ref[2] + ref[3]

    conv(0, 8)
    for g in first:
        g[1]()
    conv(8, 15)
    tok_event(0)
    for g in first:
        g[2]()
    for g in second:
        g[0]()
    conv(15, 22)
    for q in range(2):
        for lo in range(0, WIDTH, 128):
            hi = min(lo + 128, WIDTH)
            TX[x, q, :, lo:hi] = TS[q, lo:hi, :].T[0:8]
    tap_x, send_x = Group(TX.at[pl.ds(0, 3)]), family(TX.at[pl.ds(0, 3)])
    for k in (1, 2, 3):
        send_x(tap_x, TX.at[x], TX.at[x], x=ahead(x, k, 4))
    lax.fori_loop(0, 8, lambda i, _: (turn(i), 0)[1], 0)
    tok_event(1)
    wait_cross(0)
    weight_part([0], first_part=True)
    wait_cross(1, 7)
    weight_part([1, 7])
    for g in second:
        g[1]()
    tok_event(2)
    tap_x.wait()
    TY[y] = tap_sum(TX)
    tap_y, send_y = Group(TY.at[pl.ds(0, 3)]), family(TY.at[pl.ds(0, 3)])
    for k in (1, 2, 3):
        send_y(tap_y, TY.at[y], TY.at[y], y=ahead(y, k, 4))
    tok_event(3)
    for g in second:
        g[2]()
    input_part(4)
    input_part(3)
    tok_event(4)
    input_part(5)
    sum_event(0)
    sum_event(1)
    wait_cross(2, 6)
    weight_part([2, 6])
    tok_event(5)
    input_part(2)
    wait_cross(3, 5)
    weight_part([3, 5])
    tok_event(6)
    wait_cross(4)
    weight_part([4], last_part=True)
    sc_a1[0]()
    sc_b1[0]()
    input_part(6)
    sum_event(2)
    input_part(1)
    input_part(7)
    sc_a1[1]()
    sc_b1[1]()
    sum_event(3)
    input_part(0)
    tap_y.wait()
    taps = tap_sum(TY)
    diagonal = lax.broadcasted_iota(jnp.int32, (8, 128), 0) == lax.broadcasted_iota(
        jnp.int32, (8, 128), 1
    )
    NC[c] = jnp.zeros((4, 128), F32)
    for q in range(2):
        SM[8 * q : 8 * q + 8, :] = taps[q]
        square = jnp.sum(taps[q] * taps[q], axis=1, keepdims=True)
        NC[c, 2 + q : 3 + q] = jnp.sum(jnp.where(diagonal, square, 0.0), axis=0, keepdims=True)
    sum_event(4)
    sc_a1[2]()
    sc_b1[2]()
    for q in range(4):
        DA2[q] = sc_a1[3](q // 2, q % 2).astype(BF16).reshape(2, quarter, 128)
        DB2[q] = sc_b1[3](q // 2, q % 2).astype(BF16).reshape(2, quarter, 128)
    sc_a2[0]()
    sc_b2[0]()
    sc_a2[1]()
    sc_b2[1]()
    sum_event(5)
    sc_a2[2]()
    sc_b2[2]()
    for q, scat in enumerate((sc_a2, sc_b2)):
        grad = scat[3]().reshape(WIDTH, 128)
        NC[c, q : q + 1] = jnp.sum(grad * grad, axis=0, keepdims=True)
        GW[q] = grad
    pair, send_pair = Group(NC.at[0]), family(NC.at[0])
    send_pair(pair, NC.at[c], NC.at[c], c=p)
    results = [load(GW.at[0], gwg_o, 1), load(GW.at[1], vwg_o, 2)]
    pair.wait()
    NZ[z] = NC[0] + NC[1]
    along, send_along = Group(NZ.at[pl.ds(0, 7)]), family(NZ.at[pl.ds(0, 7)])
    for k in range(1, 8):
        send_along(along, NZ.at[z], NZ.at[z], z=ahead(z, k, 8))
    sum_event(6)
    partner[0].wait()
    flow[5].wait()
    pair_sum(0, 0, (1, 5), BASE)
    pair_sum(0, 1, (0, 5), BASE)
    base = load(BASE, base_o, 0)
    along.wait()
    total = NZ[0]
    for k in range(1, 8):
        total = total + NZ[k]
    SM[16:20, 0:128] = total
    small = load(SM, small_o, 3)
    for copy in (base, *results, small):
        copy.wait()
    flow[6].wait()
    for carrier, sem in sent:
        pltpu.make_async_copy(carrier, carrier, sem).wait()
    assert (next(recv_ids), next(send_ids)) == (N_RECV, N_SEND)


def finish(base, last, gwg, vwg, small, ig_o, gwg_o, vwg_o, gtg_o, vtg_o, gn_o, vn_o, tn_o):
    gwg_o[...] = gwg[...]
    vwg_o[...] = vwg[...]
    gtg_o[...] = small[0:3, :]
    vtg_o[...] = small[8:11, :]
    gn_o[...] = small[16:17, 0:128]
    vn_o[...] = small[17:18, 0:128]
    tn_o[...] = small[18:20, 0:3]
    ig_o[...] = (base[...].astype(F32) + last[...].astype(F32)).astype(BF16)


def local(tokens, up_gate, up_val, gate_weight, val_weight, gate_taps, val_taps, hidden_grad):
    hbm = pl.BlockSpec(memory_space=pl.ANY)
    vmem = pl.BlockSpec(memory_space=pltpu.VMEM)
    half = WIDTH // 2
    scratch = [
        pltpu.VMEM((8, 256, D), BF16),
        pltpu.VMEM((WIDTH, 2 * SEQ), BF16),
        pltpu.VMEM((WIDTH, 2 * SEQ), BF16),
        pltpu.VMEM((WIDTH, 2 * SEQ), BF16),
        pltpu.VMEM((3, WIDTH), BF16),
        pltpu.VMEM((3, WIDTH), BF16),
        pltpu.VMEM((24, WIDTH), F32),
        pltpu.VMEM((2, WIDTH, ROWS), F32),
        pltpu.VMEM((2, WIDTH, 128), F32),
        pltpu.VMEM((2, WIDTH, 128), F32),
        pltpu.VMEM((2 * SEQ, BOTH), BF16),
        pltpu.VMEM((8, BOTH, 256), BF16),
        pltpu.VMEM((4, 4, BOTH, ROWS), BF16),
        pltpu.VMEM((8, BOTH, 256), F32),
        pltpu.VMEM((4, 2, 2, WIDTH, 128), BF16),
        pltpu.VMEM((4, 2, 2, WIDTH, 128), BF16),
        pltpu.VMEM((4, 2, half, 128), BF16),
        pltpu.VMEM((4, 2, half, 128), BF16),
        pltpu.VMEM((2, 2, WIDTH, 128), BF16),
        pltpu.VMEM((2, 2, 2, WIDTH, 128), BF16),
        pltpu.VMEM((2, 2, WIDTH, 128), BF16),
        pltpu.VMEM((2, 2, 2, WIDTH, 128), BF16),
        pltpu.VMEM((2, half, 128), BF16),
        pltpu.VMEM((2, 2, half, 128), BF16),
        pltpu.VMEM((2, half, 128), BF16),
        pltpu.VMEM((2, 2, half, 128), BF16),
        pltpu.VMEM((8, 2, ROWS, D), BF16),
        pltpu.VMEM((8, ROWS, D), BF16),
        pltpu.VMEM((2, 7, 64, D), BF16),
        pltpu.VMEM((4, 2, 8, WIDTH), F32),
        pltpu.VMEM((4, 2, 8, WIDTH), F32),
        pltpu.VMEM((2, 4, 128), F32),
        pltpu.VMEM((8, 4, 128), F32),
        pltpu.VMEM((ROWS, D), BF16),
        pltpu.SemaphoreType.DMA((8,)),
        pltpu.SemaphoreType.DMA((N_SEND,)),
        pltpu.SemaphoreType.DMA((N_RECV,)),
    ]
    out = pl.pallas_call(
        kernel,
        out_shape=[
            jax.ShapeDtypeStruct((ROWS, D), BF16),
            jax.ShapeDtypeStruct((ROWS, D), BF16),
            jax.ShapeDtypeStruct((WIDTH, ROWS), F32),
            jax.ShapeDtypeStruct((WIDTH, ROWS), F32),
            jax.ShapeDtypeStruct((24, WIDTH), F32),
        ],
        in_specs=[hbm] * 8,
        out_specs=[hbm] * 5,
        scratch_shapes=scratch,
        compiler_params=pltpu.CompilerParams(
            collective_id=0, has_side_effects=True, vmem_limit_bytes=67_000_000
        ),
        name="backward",
    )(tokens, up_gate.T, up_val.T, gate_weight.T, val_weight.T, gate_taps, val_taps, hidden_grad.T)
    out = pl.pallas_call(
        finish,
        out_shape=[
            jax.ShapeDtypeStruct((ROWS, D), BF16),
            jax.ShapeDtypeStruct((WIDTH, ROWS), F32),
            jax.ShapeDtypeStruct((WIDTH, ROWS), F32),
            jax.ShapeDtypeStruct((3, WIDTH), F32),
            jax.ShapeDtypeStruct((3, WIDTH), F32),
            jax.ShapeDtypeStruct((1, ROWS), F32),
            jax.ShapeDtypeStruct((1, ROWS), F32),
            jax.ShapeDtypeStruct((2, 3), F32),
        ],
        in_specs=[vmem] * 5,
        out_specs=[vmem] * 8,
        name="finish",
    )(*out)
    return (out[0], out[1].T, out[2].T, out[3], out[4], out[5].reshape(ROWS), out[6].reshape(ROWS), out[7])


def solution(mesh):
    split = Mesh(mesh.devices.reshape(4, 4, 8, 2), ("y", "x", "z", "c"))
    fs, tp, both = ("y", "x"), ("z", "c"), ("y", "x", "z", "c")
    in_specs = (
        P(both, None), P(fs, tp), P(fs, tp), P(fs, tp), P(fs, tp), P(None, tp), P(None, tp), P(fs, tp),
    )
    out_specs = (
        P(both, None), P(fs, tp), P(fs, tp), P(None, tp), P(None, tp), P(fs), P(fs), P(),
    )
    return jax.shard_map(local, mesh=split, in_specs=in_specs, out_specs=out_specs, check_vma=False)
```

```python
import itertools

import jax
import jax.numpy as jnp
from jax import lax
from jax.experimental import pallas as pl
from jax.experimental.pallas import tpu as pltpu
from jax.sharding import Mesh
from jax.sharding import PartitionSpec as P

F32, BF16 = jnp.float32, jnp.bfloat16
MESH = pl.DeviceIdType.MESH
SEQ = 1024
D = 2048
ROWS = 128
WIDTH = 352
BOTH = 2 * WIDTH
GROUP = 16
TILES = SEQ // 128
NN = (((1,), (0,)), ((), ()))
N_RECV, N_SEND = 44, 12


def kernel(
    tok, ug, uv, gw, vw, gt, vt, hg,
    ig_o, gwg_o, vwg_o, gtg_o, vtg_o, gn_o, vn_o, tn_o,
    TOK, UGI, UVI, HGI, GT, VT, KT, TS, UB, UBT, W, ACC, DA, DB, DA2, DB2,
    RA0, RA1, RB0, RB1, SA0, SA1, SB0, SB1, PB, PX, RS, TX, TY, NC, NZ, BASE,
    lsem, send_sem, recv_sem,
):
    y, x, z, c = (lax.axis_index(a) for a in ("y", "x", "z", "c"))
    p = 1 - c

    def ahead(i, k, n):
        return lax.rem(i + k, n)

    recv_ids, send_ids = itertools.count(), itertools.count()
    sent = []

    class Group:
        def __init__(self, carrier):
            self.carrier = carrier
            self.sem = recv_sem.at[next(recv_ids)]

        def wait(self):
            pltpu.make_async_copy(self.carrier, self.carrier, self.sem).wait()

    def family(carrier):
        sem = send_sem.at[next(send_ids)]
        sent.append((carrier, sem))

        def remote(group, src, dst, **dev):
            pltpu.make_async_remote_copy(
                src_ref=src, dst_ref=dst, send_sem=sem, recv_sem=group.sem,
                device_id=dev, device_id_type=MESH,
            ).start()

        return remote

    def load(src, dst, i):
        copy = pltpu.make_async_copy(src, dst, lsem.at[i])
        copy.start()
        return copy

    own_rows = pl.ds(pl.multiple_of(c * ROWS, ROWS), ROWS)
    l_tok = load(tok, TOK.at[z, own_rows], 0)
    l_gw = load(gw, W.at[y, x, pl.ds(0, WIDTH)], 1)
    l_vw = load(vw, W.at[y, x, pl.ds(WIDTH, WIDTH)], 2)
    pairs = (gt, GT), (vt, VT), (ug, UGI), (uv, UVI), (hg, HGI)
    l_in = [load(a, b, 3 + i) for i, (a, b) in enumerate(pairs)]

    barrier = pltpu.get_barrier_semaphore()
    peers = [{"c": p}]
    peers += [{"x": ahead(x, k, 4)} for k in (1, 3)]
    peers += [{"y": ahead(y, k, 4)} for k in (1, 3)]
    peers += [{"z": ahead(z, k, 8)} for k in (1, 7)]
    for peer in peers:
        pl.semaphore_signal(barrier, inc=1, device_id=peer, device_id_type=MESH)

    l_tok.wait()
    pl.semaphore_wait(barrier, len(peers))

    def tok_at(zz, core, h):
        return TOK.at[zz, pl.ds(pl.multiple_of(core * ROWS + h * 64, 64), 64)]

    order_up = [(0, 0), (0, 1), (1, 0), (1, 1), (2, 0), (2, 1), (3, 0)]
    order_dn = [(s, 1 - h) for s, h in order_up]
    around, cross = {}, {}
    send_tok, send_cross = family(PB.at[pl.ds(0, 7)]), family(TOK)

    def tok_send(j):
        around[j] = Group(TOK.at[0, pl.ds(0, 128)])
        s, h = order_up[j]
        blk = tok_at(ahead(z, 8 - s, 8), c, h)
        send_tok(around[j], blk, blk, z=ahead(z, 1, 8))
        s, h = order_dn[j]
        blk = tok_at(ahead(z, s, 8), c, h)
        send_tok(around[j], blk, blk, z=ahead(z, 7, 8))

    def tok_cross(k, h):
        if k not in cross:
            alone = k in (0, 4)
            cross[k] = Group(TOK.at[0, pl.ds(0, 128)] if alone else TOK.at[0])
            if not alone:
                cross[8 - k] = cross[k]
        blk = tok_at(ahead(z, k, 8), c, h)
        send_cross(cross[k], blk, blk, c=p)

    def tok_event(j):
        around[j].wait()
        if j + 2 < 7:
            tok_send(j + 2)
        s, h = order_up[j]
        tok_cross(7 - s, h)
        s, h = order_dn[j]
        tok_cross(1 + s, h)

    tok_send(0)
    tok_send(1)
    tok_cross(0, 0)
    tok_cross(0, 1)

    def gather(remote, slot, axis, i, near_bytes, far_bytes):
        near, far = Group(near_bytes), Group(far_bytes)

        def begin():
            for s in (1, 3):
                remote(near, slot(i, None), slot(i, None), **{axis: ahead(i, s, 4)})

        def middle():
            near.wait()
            for d, s in ((0, 1), (1, 3)):
                blk = slot(ahead(i, 4 - s, 4), d)
                remote(far, blk, blk, **{axis: ahead(i, s, 4)})

        return begin, middle, far.wait

    quarter = WIDTH // 2

    def a1(i, d):
        return W.at[y, i, pl.ds(0, WIDTH) if d is None else pl.ds(quarter * d, quarter)]

    def b1(i, d):
        rows = pl.ds(WIDTH, WIDTH) if d is None else pl.ds(WIDTH + quarter * d, quarter)
        return W.at[i, x, rows]

    def a2(i, d):
        return W.at[i, pl.ds(0, 4) if d is None else pl.ds(2 * d, 2), pl.ds(0, WIDTH)]

    def b2(i, d):
        return W.at[pl.ds(0, 4) if d is None else pl.ds(2 * d, 2), i, pl.ds(WIDTH, WIDTH)]

    send_first, send_second = family(W.at[0, pl.ds(0, 3)]), family(W.at[pl.ds(0, 3)])
    near1, far1 = W.at[0, 0], W.at[0, 0, pl.ds(0, WIDTH)]
    near2, far2 = W.at[0], W.at[0, pl.ds(0, 2)]
    first = (
        gather(send_first, a1, "x", x, near1, far1),
        gather(send_first, b1, "y", y, near1, far1),
    )
    second = (
        gather(send_second, a2, "y", y, near2, far2),
        gather(send_second, b2, "x", x, near2, far2),
    )
    l_gw.wait()
    l_vw.wait()
    for g in first:
        g[0]()

    for copy in l_in:
        copy.wait()
    for q, ref in enumerate((GT, VT)):
        rows = jnp.concatenate([ref[...].astype(F32), jnp.zeros((5, WIDTH), F32)], axis=0)
        for t in range(3):
            lo, hi = t * 128, min(t * 128 + 128, WIDTH)
            KT[q, lo:hi, 0:8] = rows[:, lo:hi].T

    lane = lax.broadcasted_iota(jnp.int32, (GROUP, 128), 1)
    edge = {1: lane >= 1, 2: lane >= 2, -1: lane < 127, -2: lane < 126}
    nil = jnp.zeros((GROUP, 128), F32)

    def moved(tiles, k):
        turned = [pltpu.roll(a, k % 128, 1) for a in tiles]
        if k > 0:
            other = [nil] + turned[:-1]
        else:
            other = turned[1:] + [nil]
        return [jnp.where(edge[k], a, b) for a, b in zip(turned, other)]

    def conv(first_group, last_group):
        def step(g, _):
            rows = pl.ds(pl.multiple_of(g * GROUP, GROUP), GROUP)
            low = pl.ds(pl.multiple_of(WIDTH + g * GROUP, GROUP), GROUP)
            kg = [jnp.broadcast_to(KT[0, rows, i : i + 1], (GROUP, 128)) for i in range(3)]
            kv = [jnp.broadcast_to(KT[1, rows, i : i + 1], (GROUP, 128)) for i in range(3)]
            sums = [nil] * 6
            for s in range(2):
                at = [slice(s * SEQ + i * 128, s * SEQ + i * 128 + 128) for i in range(TILES)]
                g0 = [UGI[rows, a].astype(F32) for a in at]
                v0 = [UVI[rows, a].astype(F32) for a in at]
                g1, g2, v1, v2 = moved(g0, 1), moved(g0, 2), moved(v0, 1), moved(v0, 2)
                gb, vb = [], []
                for i in range(TILES):
                    h = HGI[rows, at[i]].astype(F32)
                    cg = kg[0] * g2[i] + kg[1] * g1[i] + kg[2] * g0[i]
                    cv = kv[0] * v2[i] + kv[1] * v1[i] + kv[2] * v0[i]
                    sg = jax.nn.sigmoid(cg)
                    hs = h * sg
                    vb.append(hs * cg)
                    gb.append(hs * cv * (1.0 + cg * (1.0 - sg)))
                    terms = [u * gb[i] for u in (g2[i], g1[i], g0[i])]
                    terms += [u * vb[i] for u in (v2[i], v1[i], v0[i])]
                    sums = [a + b for a, b in zip(sums, terms)]
                gb1, gb2, vb1, vb2 = moved(gb, -1), moved(gb, -2), moved(vb, -1), moved(vb, -2)
                for i in range(TILES):
                    half = slice((i % 2) * 128, (i % 2) * 128 + 128)
                    og = kg[2] * gb[i] + kg[1] * gb1[i] + kg[0] * gb2[i]
                    ov = kv[2] * vb[i] + kv[1] * vb1[i] + kv[0] * vb2[i]
                    UBT[4 * s + i // 2, rows, half] = og.astype(BF16)
                    UBT[4 * s + i // 2, low, half] = ov.astype(BF16)
            for q in range(2):
                t = [jnp.sum(sums[3 * q + i], axis=1, keepdims=True) for i in range(3)]
                TS[q, rows, :] = jnp.where(
                    lane == 0, t[0], jnp.where(lane == 1, t[1], jnp.where(lane == 2, t[2], 0.0))
                )
            return 0

        lax.fori_loop(first_group, last_group, step, 0)

    def turn(zz):
        rows = pl.ds(pl.multiple_of(zz * 256, 256), 256)
        for lo in range(0, BOTH, 128):
            hi = min(lo + 128, BOTH)
            UB[rows, lo:hi] = UBT[zz, lo:hi, :].T

    def weight_part(ks, first_part=False, last_part=False):
        zs = [ahead(z, k, 8) for k in ks]

        def step(n, _):
            cols = pl.ds(pl.multiple_of(n * 256, 256), 256)
            total = None
            for zz in zs:
                part = lax.dot_general(UBT[zz], TOK[zz, :, cols], NN, preferred_element_type=F32)
                total = part if total is None else total + part
            if not first_part:
                total = total + ACC[n]
            if last_part:
                out = total.astype(BF16)
                yy, xx = n // 2, 2 * (n % 2)
                for q in range(2):
                    DA[xx + q, yy // 2, yy % 2] = out[0:WIDTH, q * 128 : q * 128 + 128]
                    DB[yy, xx // 2, q] = out[WIDTH:BOTH, q * 128 : q * 128 + 128]
            else:
                ACC[n] = total
            return 0

        lax.fori_loop(0, 8, step, 0)

    def wait_cross(*ks):
        for group in {id(cross[k]): cross[k] for k in ks}.values():
            group.wait()

    partner = {}
    send_part = send_cross

    def input_part(k):
        zz = ahead(z, k, 8)
        rows = pl.ds(pl.multiple_of(zz * 256, 256), 256)

        def step(n, _):
            yy, xx = n // 2, 2 * (n % 2)
            w = jnp.concatenate([W[yy, xx], W[yy, xx + 1]], axis=1)
            out = lax.dot_general(UB[rows, :], w, NN, preferred_element_type=F32).astype(BF16)
            cols = pl.ds(pl.multiple_of(n * 256, 256), 256)
            PB[k, 0, :, cols] = out[0:128]
            PB[k, 1, :, cols] = out[128:256]
            return 0

        lax.fori_loop(0, 8, step, 0)
        if k not in partner:
            alone = k in (0, 4)
            partner[k] = Group(PX.at[0] if alone else PX.at[pl.ds(0, 2)])
            if not alone:
                partner[8 - k] = partner[k]
        send_part(partner[k], PB.at[k, p], PX.at[k], c=p)

    sum_up = [(0, 0), (1, 1), (1, 0), (2, 1), (2, 0), (3, 1), (3, 0)]
    flow = {}
    send_flow = send_tok

    def pair_sum(k, h, extra, dst=None):
        def step(i, _):
            rows = pl.ds(pl.multiple_of(h * 64 + i * 16, 16), 16)
            v = PB[k, c, rows, :].astype(F32) + PX[k, rows, :].astype(F32)
            if extra is not None:
                v = v + RS[extra[0], extra[1], pl.ds(pl.multiple_of(i * 16, 16), 16), :].astype(F32)
            if dst is None:
                PB[k, c, rows, :] = v.astype(BF16)
            else:
                dst[rows, :] = v.astype(BF16)
            return 0

        lax.fori_loop(0, 4, step, 0)

    def sum_event(j):
        s = sum_up[j][0]
        ks = (4 - s, 4 + s)
        if j in (0, 1, 3, 5):
            partner[ks[0]].wait()
        if j >= 2:
            flow[j - 2].wait()
        flow[j] = Group(TOK.at[0, pl.ds(0, 128)])
        for d in range(2):
            h = sum_up[j][1] if d == 0 else 1 - sum_up[j][1]
            pair_sum(ks[d], h, (d, j - 2) if j >= 2 else None)
            send_flow(
                flow[j],
                PB.at[ks[d], c, pl.ds(h * 64, 64)],
                RS.at[d, j],
                z=ahead(z, 1 if d == 0 else 7, 8),
            )

    def scatter(src, r0, r1, axis, i):
        own = i
        near = {0: ahead(i, 1, 4), 1: ahead(i, 3, 4)}
        far = ahead(i, 2, 4)
        remote = family(src.at[pl.ds(0, 3)])
        early, late = Group(r0), Group(r1)

        def begin():
            for d in range(2):
                to = {axis: near[d]}
                remote(early, src.at[far, d], r0.at[d], **to)
                remote(late, src.at[near[d], 1 - d], r1.at[d, 1 - d], **to)

        def middle():
            early.wait()
            for d in range(2):
                src[near[d], d] = (src[near[d], d].astype(F32) + r0[d].astype(F32)).astype(BF16)
                remote(late, src.at[near[d], d], r1.at[d, d], **{axis: near[d]})

        end = late.wait

        def total(*at):
            t = src[(own, *at)].astype(F32)
            return t + r1[(0, *at)].astype(F32) + r1[(1, *at)].astype(F32)

        return begin, middle, end, total

    sc_a1 = scatter(DA, RA0, RA1, "x", x)
    sc_b1 = scatter(DB, RB0, RB1, "y", y)
    sc_a2 = scatter(DA2, SA0, SA1, "y", y)
    sc_b2 = scatter(DB2, SB0, SB1, "x", x)

    def tap_sum(ref):
        return ref[0] + ref[1] + ref[2] + ref[3]

    conv(0, 8)
    for g in first:
        g[1]()
    conv(8, 15)
    tok_event(0)
    for g in first:
        g[2]()
    for g in second:
        g[0]()
    conv(15, 22)
    for q in range(2):
        for lo in range(0, WIDTH, 128):
            hi = min(lo + 128, WIDTH)
            TX[x, q, :, lo:hi] = TS[q, lo:hi, :].T[0:8]
    tap_x, send_x = Group(TX.at[pl.ds(0, 3)]), family(TX.at[pl.ds(0, 3)])
    for k in (1, 2, 3):
        send_x(tap_x, TX.at[x], TX.at[x], x=ahead(x, k, 4))
    lax.fori_loop(0, 8, lambda i, _: (turn(i), 0)[1], 0)
    tok_event(1)
    wait_cross(0)
    weight_part([0], first_part=True)
    wait_cross(1, 7)
    weight_part([1, 7])
    for g in second:
        g[1]()
    tok_event(2)
    tap_x.wait()
    TY[y] = tap_sum(TX)
    tap_y, send_y = Group(TY.at[pl.ds(0, 3)]), family(TY.at[pl.ds(0, 3)])
    for k in (1, 2, 3):
        send_y(tap_y, TY.at[y], TY.at[y], y=ahead(y, k, 4))
    tok_event(3)
    for g in second:
        g[2]()
    input_part(4)
    input_part(3)
    tok_event(4)
    input_part(5)
    sum_event(0)
    sum_event(1)
    wait_cross(2, 6)
    weight_part([2, 6])
    tok_event(5)
    input_part(2)
    wait_cross(3, 5)
    weight_part([3, 5])
    tok_event(6)
    wait_cross(4)
    weight_part([4], last_part=True)
    sc_a1[0]()
    sc_b1[0]()
    input_part(6)
    sum_event(2)
    input_part(1)
    input_part(7)
    sc_a1[1]()
    sc_b1[1]()
    sum_event(3)
    input_part(0)
    tap_y.wait()
    taps = tap_sum(TY)
    diagonal = lax.broadcasted_iota(jnp.int32, (8, 128), 0) == lax.broadcasted_iota(
        jnp.int32, (8, 128), 1
    )
    NC[c] = jnp.zeros((4, 128), F32)
    for q in range(2):
        (gtg_o, vtg_o)[q][...] = taps[q, 0:3]
        square = jnp.sum(taps[q] * taps[q], axis=1, keepdims=True)
        NC[c, 2 + q : 3 + q] = jnp.sum(jnp.where(diagonal, square, 0.0), axis=0, keepdims=True)
    sum_event(4)
    sc_a1[2]()
    sc_b1[2]()
    for q in range(4):
        DA2[q] = sc_a1[3](q // 2, q % 2).astype(BF16).reshape(2, quarter, 128)
        DB2[q] = sc_b1[3](q // 2, q % 2).astype(BF16).reshape(2, quarter, 128)
    sc_a2[0]()
    sc_b2[0]()
    sc_a2[1]()
    sc_b2[1]()
    sum_event(5)
    sc_a2[2]()
    sc_b2[2]()
    for q, scat in enumerate((sc_a2, sc_b2)):
        grad = scat[3]().reshape(WIDTH, 128)
        NC[c, q : q + 1] = jnp.sum(grad * grad, axis=0, keepdims=True)
        (gwg_o, vwg_o)[q][...] = grad
    pair, send_pair = Group(NC.at[0]), family(NC.at[0])
    send_pair(pair, NC.at[c], NC.at[c], c=p)
    pair.wait()
    NZ[z] = NC[0] + NC[1]
    along, send_along = Group(NZ.at[pl.ds(0, 7)]), family(NZ.at[pl.ds(0, 7)])
    for k in range(1, 8):
        send_along(along, NZ.at[z], NZ.at[z], z=ahead(z, k, 8))
    sum_event(6)
    partner[0].wait()
    flow[5].wait()
    pair_sum(0, 0, (1, 5), BASE)
    pair_sum(0, 1, (0, 5), BASE)
    along.wait()
    total = NZ[0]
    for k in range(1, 8):
        total = total + NZ[k]
    gn_o[...] = total[0:1]
    vn_o[...] = total[1:2]
    tn_o[...] = total[2:4, 0:3]
    flow[6].wait()

    def last(i, _):
        for d in range(2):
            rows = pl.ds(pl.multiple_of(d * 64 + i * 16, 16), 16)
            here = pl.ds(pl.multiple_of(i * 16, 16), 16)
            ig_o[rows, :] = (BASE[rows, :].astype(F32) + RS[d, 6, here, :].astype(F32)).astype(BF16)
        return 0

    lax.fori_loop(0, 4, last, 0)
    for carrier, sem in sent:
        pltpu.make_async_copy(carrier, carrier, sem).wait()
    assert (next(recv_ids), next(send_ids)) == (N_RECV, N_SEND)


def finish(*refs):
    srcs, dsts, sem = refs[:8], refs[8:16], refs[16]
    copies = [pltpu.make_async_copy(a, b, sem.at[i]) for i, (a, b) in enumerate(zip(srcs, dsts))]
    for c in copies:
        c.start()
    for c in copies:
        c.wait()


def local(tokens, up_gate, up_val, gate_weight, val_weight, gate_taps, val_taps, hidden_grad):
    hbm = pl.BlockSpec(memory_space=pl.ANY)
    half = WIDTH // 2
    scratch = [
        pltpu.VMEM((8, 256, D), BF16),
        pltpu.VMEM((WIDTH, 2 * SEQ), BF16),
        pltpu.VMEM((WIDTH, 2 * SEQ), BF16),
        pltpu.VMEM((WIDTH, 2 * SEQ), BF16),
        pltpu.VMEM((3, WIDTH), BF16),
        pltpu.VMEM((3, WIDTH), BF16),
        pltpu.VMEM((2, WIDTH, 128), F32),
        pltpu.VMEM((2, WIDTH, 128), F32),
        pltpu.VMEM((2 * SEQ, BOTH), BF16),
        pltpu.VMEM((8, BOTH, 256), BF16),
        pltpu.VMEM((4, 4, BOTH, ROWS), BF16),
        pltpu.VMEM((8, BOTH, 256), F32),
        pltpu.VMEM((4, 2, 2, WIDTH, 128), BF16),
        pltpu.VMEM((4, 2, 2, WIDTH, 128), BF16),
        pltpu.VMEM((4, 2, half, 128), BF16),
        pltpu.VMEM((4, 2, half, 128), BF16),
        pltpu.VMEM((2, 2, WIDTH, 128), BF16),
        pltpu.VMEM((2, 2, 2, WIDTH, 128), BF16),
        pltpu.VMEM((2, 2, WIDTH, 128), BF16),
        pltpu.VMEM((2, 2, 2, WIDTH, 128), BF16),
        pltpu.VMEM((2, half, 128), BF16),
        pltpu.VMEM((2, 2, half, 128), BF16),
        pltpu.VMEM((2, half, 128), BF16),
        pltpu.VMEM((2, 2, half, 128), BF16),
        pltpu.VMEM((8, 2, ROWS, D), BF16),
        pltpu.VMEM((8, ROWS, D), BF16),
        pltpu.VMEM((2, 7, 64, D), BF16),
        pltpu.VMEM((4, 2, 8, WIDTH), F32),
        pltpu.VMEM((4, 2, 8, WIDTH), F32),
        pltpu.VMEM((2, 4, 128), F32),
        pltpu.VMEM((8, 4, 128), F32),
        pltpu.VMEM((ROWS, D), BF16),
        pltpu.SemaphoreType.DMA((8,)),
        pltpu.SemaphoreType.DMA((N_SEND,)),
        pltpu.SemaphoreType.DMA((N_RECV,)),
    ]
    shapes = [
        jax.ShapeDtypeStruct((ROWS, D), BF16),
        jax.ShapeDtypeStruct((WIDTH, ROWS), F32),
        jax.ShapeDtypeStruct((WIDTH, ROWS), F32),
        jax.ShapeDtypeStruct((3, WIDTH), F32),
        jax.ShapeDtypeStruct((3, WIDTH), F32),
        jax.ShapeDtypeStruct((1, ROWS), F32),
        jax.ShapeDtypeStruct((1, ROWS), F32),
        jax.ShapeDtypeStruct((2, 3), F32),
    ]
    vmem = pl.BlockSpec(memory_space=pltpu.VMEM)
    args = (
        tokens, up_gate.T, up_val.T, gate_weight.T, val_weight.T, gate_taps, val_taps, hidden_grad.T,
    )
    kept = [pltpu.with_memory_space_constraint(a, pltpu.HBM) for a in args]
    out = pl.pallas_call(
        kernel,
        out_shape=shapes,
        in_specs=[hbm] * 8,
        out_specs=[vmem] * 8,
        scratch_shapes=scratch,
        compiler_params=pltpu.CompilerParams(
            collective_id=0, has_side_effects=True, vmem_limit_bytes=54000000
        ),
        name="backward",
    )(*kept)
    out = pl.pallas_call(
        finish,
        out_shape=shapes,
        in_specs=[vmem] * 8,
        out_specs=[hbm] * 8,
        scratch_shapes=[pltpu.SemaphoreType.DMA((8,))],
        compiler_params=pltpu.CompilerParams(vmem_limit_bytes=4_000_000),
        name="finish",
    )(*out)
    return (out[0], out[1].T, out[2].T, out[3], out[4], out[5].reshape(ROWS), out[6].reshape(ROWS), out[7])


def solution(mesh):
    split = Mesh(mesh.devices.reshape(4, 4, 8, 2), ("y", "x", "z", "c"))
    fs, tp, both = ("y", "x"), ("z", "c"), ("y", "x", "z", "c")
    in_specs = (
        P(both, None), P(fs, tp), P(fs, tp), P(fs, tp), P(fs, tp), P(None, tp), P(None, tp), P(fs, tp),
    )
    out_specs = (
        P(both, None), P(fs, tp), P(fs, tp), P(None, tp), P(None, tp), P(fs), P(fs), P(),
    )
    return jax.shard_map(local, mesh=split, in_specs=in_specs, out_specs=out_specs, check_vma=False)
```

```python
import itertools

import jax
import jax.numpy as jnp
from jax import lax
from jax.experimental import pallas as pl
from jax.experimental.pallas import tpu as pltpu
from jax.sharding import Mesh
from jax.sharding import PartitionSpec as P

F32, BF16 = jnp.float32, jnp.bfloat16
MESH = pl.DeviceIdType.MESH
SEQ = 1024
D = 2048
ROWS = 128
WIDTH = 352
BOTH = 2 * WIDTH
GROUP = 16
TILES = SEQ // 128
NN = (((1,), (0,)), ((), ()))
N_RECV, N_SEND = 44, 14


def kernel(
    tok, ug, uv, gw, vw, gt, vt, hg,
    ig_o, gwg_o, vwg_o, gtg_o, vtg_o, gn_o, vn_o, tn_o,
    TOK, UGI, UVI, HGI, GT, VT, KT, TS, UB, UBT, W, ACC, DA, DB, DA2, DB2,
    RA0, RA1, RB0, RB1, SA0, SA1, SB0, SB1, PB, PX, RS, TX, TY, NC, NZ, BASE,
    lsem, send_sem, recv_sem,
):
    y, x, z, c = (lax.axis_index(a) for a in ("y", "x", "z", "c"))
    p = 1 - c

    def ahead(i, k, n):
        return lax.rem(i + k, n)

    recv_ids, send_ids = itertools.count(), itertools.count()
    sent = []

    class Group:
        def __init__(self, carrier):
            self.carrier = carrier
            self.sem = recv_sem.at[next(recv_ids)]

        def wait(self):
            pltpu.make_async_copy(self.carrier, self.carrier, self.sem).wait()

    def family(carrier):
        sem = send_sem.at[next(send_ids)]
        sent.append((carrier, sem))

        return sender(sem)

    def sender(sem):
        def remote(group, src, dst, **dev):
            pltpu.make_async_remote_copy(
                src_ref=src, dst_ref=dst, send_sem=sem, recv_sem=group.sem,
                device_id=dev, device_id_type=MESH,
            ).start()

        return remote

    def load(src, dst, i):
        copy = pltpu.make_async_copy(src, dst, lsem.at[i])
        copy.start()
        return copy

    own_rows = pl.ds(pl.multiple_of(c * ROWS, ROWS), ROWS)
    l_tok = load(tok, TOK.at[z, own_rows], 0)
    l_gw = load(gw, W.at[y, x, pl.ds(0, WIDTH)], 1)
    l_vw = load(vw, W.at[y, x, pl.ds(WIDTH, WIDTH)], 2)
    pairs = (gt, GT), (vt, VT), (ug, UGI), (uv, UVI), (hg, HGI)
    l_in = [load(a, b, 3 + i) for i, (a, b) in enumerate(pairs)]

    barrier = pltpu.get_barrier_semaphore()
    peers = [{"c": p}]
    peers += [{"x": ahead(x, k, 4)} for k in (1, 3)]
    peers += [{"y": ahead(y, k, 4)} for k in (1, 3)]
    peers += [{"z": ahead(z, k, 8)} for k in (1, 7)]
    for peer in peers:
        pl.semaphore_signal(barrier, inc=1, device_id=peer, device_id_type=MESH)

    l_tok.wait()
    pl.semaphore_wait(barrier, len(peers))

    def tok_at(zz, core, h):
        return TOK.at[zz, pl.ds(pl.multiple_of(core * ROWS + h * 64, 64), 64)]

    order_up = [(0, 0), (0, 1), (1, 0), (1, 1), (2, 0), (2, 1), (3, 0)]
    order_dn = [(s, 1 - h) for s, h in order_up]
    around, cross = {}, {}
    send_tok, send_cross = family(RS.at[pl.ds(0, 2), pl.ds(0, 6)]), family(TOK)

    edge_sem = send_sem.at[next(send_ids)]
    send_edge = sender(edge_sem)

    def tok_last():
        around[6] = Group(TOK.at[0, pl.ds(0, 128)])
        blk = tok_at(ahead(z, 3, 8), c, 1)
        send_edge(around[6], blk, blk, z=ahead(z, 7, 8))
        zz, top = ahead(z, 5, 8), pl.multiple_of(c * ROWS, ROWS)
        blk = TOK.at[zz, pl.ds(top, 48)]
        send_edge(around[6], blk, blk, z=ahead(z, 1, 8))

        @pl.when(z != 7)
        def _():
            rest = TOK.at[zz, pl.ds(pl.multiple_of(top + 48, 16), 16)]
            send_edge(around[6], rest, rest, z=ahead(z, 1, 8))

    def tok_extra():
        @pl.when(z == 1)
        def _():
            rest = TOK.at[ahead(z, 3, 8), pl.ds(pl.multiple_of(c * ROWS + 48, 16), 16)]
            send_edge(around[6], rest, rest, z=ahead(z, 7, 8))

    def tok_last_wait():
        for case, rows in ((z == 7, 112), (z == 1, 144), ((z != 7) & (z != 1), 128)):

            @pl.when(case)
            def _(rows=rows):
                blk = TOK.at[0, pl.ds(0, rows)]
                pltpu.make_async_copy(blk, blk, edge_sem).wait()

    def tok_send(j):
        if j == 6:
            tok_last()
            return
        around[j] = Group(TOK.at[0, pl.ds(0, 128)])
        s, h = order_up[j]
        blk = tok_at(ahead(z, 8 - s, 8), c, h)
        send_tok(around[j], blk, blk, z=ahead(z, 1, 8))
        s, h = order_dn[j]
        blk = tok_at(ahead(z, s, 8), c, h)
        send_tok(around[j], blk, blk, z=ahead(z, 7, 8))

    def tok_cross(k, h):
        if k not in cross:
            alone = k in (0, 4)
            cross[k] = Group(TOK.at[0, pl.ds(0, 128)] if alone else TOK.at[0])
            if not alone:
                cross[8 - k] = cross[k]
        blk = tok_at(ahead(z, k, 8), c, h)
        send_cross(cross[k], blk, blk, c=p)

    def tok_event(j):
        around[j].wait()
        if j + 2 < 7:
            tok_send(j + 2)
        if j == 5:
            tok_extra()
        s, h = order_up[j]
        tok_cross(7 - s, h)
        s, h = order_dn[j]
        tok_cross(1 + s, h)

    tok_send(0)
    tok_send(1)
    tok_cross(0, 0)
    tok_cross(0, 1)

    def gather(remote, slot, axis, i, near_bytes, far_bytes):
        near, far = Group(near_bytes), Group(far_bytes)

        def begin():
            for s in (1, 3):
                remote(near, slot(i, None), slot(i, None), **{axis: ahead(i, s, 4)})

        def middle():
            near.wait()
            for d, s in ((0, 1), (1, 3)):
                blk = slot(ahead(i, 4 - s, 4), d)
                remote(far, blk, blk, **{axis: ahead(i, s, 4)})

        return begin, middle, far.wait

    quarter = WIDTH // 2

    def a1(i, d):
        return W.at[y, i, pl.ds(0, WIDTH) if d is None else pl.ds(quarter * d, quarter)]

    def b1(i, d):
        rows = pl.ds(WIDTH, WIDTH) if d is None else pl.ds(WIDTH + quarter * d, quarter)
        return W.at[i, x, rows]

    def a2(i, d):
        return W.at[i, pl.ds(0, 4) if d is None else pl.ds(2 * d, 2), pl.ds(0, WIDTH)]

    def b2(i, d):
        return W.at[pl.ds(0, 4) if d is None else pl.ds(2 * d, 2), i, pl.ds(WIDTH, WIDTH)]

    send_first, send_second = family(W.at[0, pl.ds(0, 3)]), family(W.at[pl.ds(0, 3)])
    near1, far1 = W.at[0, 0], W.at[0, 0, pl.ds(0, WIDTH)]
    near2, far2 = W.at[0], W.at[0, pl.ds(0, 2)]
    first = (
        gather(send_first, a1, "x", x, near1, far1),
        gather(send_first, b1, "y", y, near1, far1),
    )
    second = (
        gather(send_second, a2, "y", y, near2, far2),
        gather(send_second, b2, "x", x, near2, far2),
    )
    l_gw.wait()
    l_vw.wait()
    for g in first:
        g[0]()

    for copy in l_in:
        copy.wait()
    for q, ref in enumerate((GT, VT)):
        rows = jnp.concatenate([ref[...].astype(F32), jnp.zeros((5, WIDTH), F32)], axis=0)
        for t in range(3):
            lo, hi = t * 128, min(t * 128 + 128, WIDTH)
            KT[q, lo:hi, 0:8] = rows[:, lo:hi].T

    lane = lax.broadcasted_iota(jnp.int32, (GROUP, 128), 1)
    edge = {1: lane >= 1, 2: lane >= 2, -1: lane < 127, -2: lane < 126}
    nil = jnp.zeros((GROUP, 128), F32)

    def moved(tiles, k):
        turned = [pltpu.roll(a, k % 128, 1) for a in tiles]
        if k > 0:
            other = [nil] + turned[:-1]
        else:
            other = turned[1:] + [nil]
        return [jnp.where(edge[k], a, b) for a, b in zip(turned, other)]

    def conv(first_group, last_group):
        def step(g, _):
            rows = pl.ds(pl.multiple_of(g * GROUP, GROUP), GROUP)
            low = pl.ds(pl.multiple_of(WIDTH + g * GROUP, GROUP), GROUP)
            kg = [jnp.broadcast_to(KT[0, rows, i : i + 1], (GROUP, 128)) for i in range(3)]
            kv = [jnp.broadcast_to(KT[1, rows, i : i + 1], (GROUP, 128)) for i in range(3)]
            sums = [nil] * 6
            for s in range(2):
                at = [slice(s * SEQ + i * 128, s * SEQ + i * 128 + 128) for i in range(TILES)]
                g0 = [UGI[rows, a].astype(F32) for a in at]
                v0 = [UVI[rows, a].astype(F32) for a in at]
                g1, g2, v1, v2 = moved(g0, 1), moved(g0, 2), moved(v0, 1), moved(v0, 2)
                gb, vb = [], []
                for i in range(TILES):
                    h = HGI[rows, at[i]].astype(F32)
                    cg = kg[0] * g2[i] + kg[1] * g1[i] + kg[2] * g0[i]
                    cv = kv[0] * v2[i] + kv[1] * v1[i] + kv[2] * v0[i]
                    sg = jax.nn.sigmoid(cg)
                    hs = h * sg
                    vb.append(hs * cg)
                    gb.append(hs * cv * (1.0 + cg * (1.0 - sg)))
                    terms = [u * gb[i] for u in (g2[i], g1[i], g0[i])]
                    terms += [u * vb[i] for u in (v2[i], v1[i], v0[i])]
                    sums = [a + b for a, b in zip(sums, terms)]
                gb1, gb2, vb1, vb2 = moved(gb, -1), moved(gb, -2), moved(vb, -1), moved(vb, -2)
                for i in range(TILES):
                    half = slice((i % 2) * 128, (i % 2) * 128 + 128)
                    og = kg[2] * gb[i] + kg[1] * gb1[i] + kg[0] * gb2[i]
                    ov = kv[2] * vb[i] + kv[1] * vb1[i] + kv[0] * vb2[i]
                    UBT[4 * s + i // 2, rows, half] = og.astype(BF16)
                    UBT[4 * s + i // 2, low, half] = ov.astype(BF16)
            for q in range(2):
                t = [jnp.sum(sums[3 * q + i], axis=1, keepdims=True) for i in range(3)]
                TS[q, rows, :] = jnp.where(
                    lane == 0, t[0], jnp.where(lane == 1, t[1], jnp.where(lane == 2, t[2], 0.0))
                )
            return 0

        lax.fori_loop(first_group, last_group, step, 0)

    def turn(zz):
        rows = pl.ds(pl.multiple_of(zz * 256, 256), 256)
        for lo in range(0, BOTH, 128):
            hi = min(lo + 128, BOTH)
            UB[rows, lo:hi] = UBT[zz, lo:hi, :].T

    def weight_part(ks, first_part=False, last_part=False):
        zs = [ahead(z, k, 8) for k in ks]

        def step(n, _):
            cols = pl.ds(pl.multiple_of(n * 256, 256), 256)
            total = None
            for zz in zs:
                part = lax.dot_general(UBT[zz], TOK[zz, :, cols], NN, preferred_element_type=F32)
                total = part if total is None else total + part
            if not first_part:
                total = total + ACC[n]
            if last_part:
                out = total.astype(BF16)
                yy, xx = n // 2, 2 * (n % 2)
                for q in range(2):
                    DA[xx + q, yy // 2, yy % 2] = out[0:WIDTH, q * 128 : q * 128 + 128]
                    DB[yy, xx // 2, q] = out[WIDTH:BOTH, q * 128 : q * 128 + 128]
            else:
                ACC[n] = total
            return 0

        lax.fori_loop(0, 8, step, 0)

    def wait_cross(*ks):
        for group in {id(cross[k]): cross[k] for k in ks}.values():
            group.wait()

    partner = {}
    send_part = send_cross

    def input_part(k):
        zz = ahead(z, k, 8)
        rows = pl.ds(pl.multiple_of(zz * 256, 256), 256)

        def step(n, _):
            yy, xx = n // 2, 2 * (n % 2)
            w = jnp.concatenate([W[yy, xx], W[yy, xx + 1]], axis=1)
            out = lax.dot_general(UB[rows, :], w, NN, preferred_element_type=F32).astype(BF16)
            cols = pl.ds(pl.multiple_of(n * 256, 256), 256)
            PB[k, 0, :, cols] = out[0:128]
            PB[k, 1, :, cols] = out[128:256]
            return 0

        lax.fori_loop(0, 8, step, 0)
        if k not in partner:
            alone = k in (0, 4)
            partner[k] = Group(PX.at[0] if alone else PX.at[pl.ds(0, 2)])
            if not alone:
                partner[8 - k] = partner[k]
        send_part(partner[k], PB.at[k, p], PX.at[k], c=p)

    sum_up = [(0, 0), (1, 1), (1, 0), (2, 1), (2, 0), (3, 1), (3, 0)]
    flow = {}
    send_flow = family(RS)

    def pair_sum(k, h, extra, dst=None):
        def step(i, _):
            rows = pl.ds(pl.multiple_of(h * 64 + i * 16, 16), 16)
            v = PB[k, c, rows, :].astype(F32) + PX[k, rows, :].astype(F32)
            if extra is not None:
                v = v + RS[extra[0], extra[1], pl.ds(pl.multiple_of(i * 16, 16), 16), :].astype(F32)
            if dst is None:
                PB[k, c, rows, :] = v.astype(BF16)
            else:
                dst[rows, :] = v.astype(BF16)
            return 0

        lax.fori_loop(0, 4, step, 0)

    def sum_event(j):
        s = sum_up[j][0]
        ks = (4 - s, 4 + s)
        if j in (0, 1, 3, 5):
            partner[ks[0]].wait()
        if j >= 2:
            flow[j - 2].wait()
        flow[j] = Group(TOK.at[0, pl.ds(0, 128)])
        for d in range(2):
            h = sum_up[j][1] if d == 0 else 1 - sum_up[j][1]
            pair_sum(ks[d], h, (d, j - 2) if j >= 2 else None)
            send_flow(
                flow[j],
                PB.at[ks[d], c, pl.ds(h * 64, 64)],
                RS.at[d, j],
                z=ahead(z, 1 if d == 0 else 7, 8),
            )

    def scatter(src, r0, r1, axis, i):
        own = i
        near = {0: ahead(i, 1, 4), 1: ahead(i, 3, 4)}
        far = ahead(i, 2, 4)
        remote = family(src.at[pl.ds(0, 3)])
        early, late = Group(r0), Group(r1)

        def begin():
            for d in range(2):
                to = {axis: near[d]}
                remote(early, src.at[far, d], r0.at[d], **to)
                remote(late, src.at[near[d], 1 - d], r1.at[d, 1 - d], **to)

        def middle():
            early.wait()
            for d in range(2):
                src[near[d], d] = (src[near[d], d].astype(F32) + r0[d].astype(F32)).astype(BF16)
                remote(late, src.at[near[d], d], r1.at[d, d], **{axis: near[d]})

        end = late.wait

        def total(*at):
            t = src[(own, *at)].astype(F32)
            return t + r1[(0, *at)].astype(F32) + r1[(1, *at)].astype(F32)

        return begin, middle, end, total

    sc_a1 = scatter(DA, RA0, RA1, "x", x)
    sc_b1 = scatter(DB, RB0, RB1, "y", y)
    sc_a2 = scatter(DA2, SA0, SA1, "y", y)
    sc_b2 = scatter(DB2, SB0, SB1, "x", x)

    def tap_sum(ref):
        return ref[0] + ref[1] + ref[2] + ref[3]

    conv(0, 8)
    for g in first:
        g[1]()
    conv(8, 15)
    tok_event(0)
    for g in first:
        g[2]()
    for g in second:
        g[0]()
    conv(15, 22)
    for q in range(2):
        for lo in range(0, WIDTH, 128):
            hi = min(lo + 128, WIDTH)
            TX[x, q, :, lo:hi] = TS[q, lo:hi, :].T[0:8]
    tap_x, send_x = Group(TX.at[pl.ds(0, 3)]), family(TX.at[pl.ds(0, 3)])
    for k in (1, 2, 3):
        send_x(tap_x, TX.at[x], TX.at[x], x=ahead(x, k, 4))
    lax.fori_loop(0, 8, lambda i, _: (turn(i), 0)[1], 0)
    tok_event(1)
    wait_cross(0)
    weight_part([0], first_part=True)
    wait_cross(1, 7)
    weight_part([1, 7])
    for g in second:
        g[1]()
    tok_event(2)
    tap_x.wait()
    TY[y] = tap_sum(TX)
    tap_y, send_y = Group(TY.at[pl.ds(0, 3)]), family(TY.at[pl.ds(0, 3)])
    for k in (1, 2, 3):
        send_y(tap_y, TY.at[y], TY.at[y], y=ahead(y, k, 4))
    tok_event(3)
    for g in second:
        g[2]()
    input_part(4)
    input_part(3)
    tok_event(4)
    input_part(5)
    sum_event(0)
    sum_event(1)
    wait_cross(2, 6)
    weight_part([2, 6])
    tok_event(5)
    input_part(2)
    wait_cross(3, 5)
    weight_part([3, 5])
    tok_event(6)
    wait_cross(4)
    weight_part([4], last_part=True)
    sc_a1[0]()
    sc_b1[0]()
    input_part(6)
    sum_event(2)
    input_part(1)
    input_part(7)
    sc_a1[1]()
    sc_b1[1]()
    sum_event(3)
    input_part(0)
    tap_y.wait()
    taps = tap_sum(TY)
    diagonal = lax.broadcasted_iota(jnp.int32, (8, 128), 0) == lax.broadcasted_iota(
        jnp.int32, (8, 128), 1
    )
    NC[c] = jnp.zeros((4, 128), F32)
    for q in range(2):
        (gtg_o, vtg_o)[q][...] = taps[q, 0:3]
        square = jnp.sum(taps[q] * taps[q], axis=1, keepdims=True)
        NC[c, 2 + q : 3 + q] = jnp.sum(jnp.where(diagonal, square, 0.0), axis=0, keepdims=True)
    sum_event(4)
    sc_a1[2]()
    sc_b1[2]()
    for q in range(4):
        DA2[q] = sc_a1[3](q // 2, q % 2).astype(BF16).reshape(2, quarter, 128)
        DB2[q] = sc_b1[3](q // 2, q % 2).astype(BF16).reshape(2, quarter, 128)
    sc_a2[0]()
    sc_b2[0]()
    sc_a2[1]()
    sc_b2[1]()
    sum_event(5)
    sc_a2[2]()
    sc_b2[2]()
    for q, scat in enumerate((sc_a2, sc_b2)):
        grad = scat[3]().reshape(WIDTH, 128)
        NC[c, q : q + 1] = jnp.sum(grad * grad, axis=0, keepdims=True)
        (gwg_o, vwg_o)[q][...] = grad
    pair, send_pair = Group(NC.at[0]), family(NC.at[0])
    send_pair(pair, NC.at[c], NC.at[c], c=p)
    pair.wait()
    NZ[z] = NC[0] + NC[1]
    along, send_along = Group(NZ.at[pl.ds(0, 7)]), family(NZ.at[pl.ds(0, 7)])
    for k in range(1, 8):
        send_along(along, NZ.at[z], NZ.at[z], z=ahead(z, k, 8))
    sum_event(6)
    partner[0].wait()
    flow[5].wait()
    pair_sum(0, 0, (1, 5), BASE)
    pair_sum(0, 1, (0, 5), BASE)
    along.wait()
    total = NZ[0]
    for k in range(1, 8):
        total = total + NZ[k]
    gn_o[...] = total[0:1]
    vn_o[...] = total[1:2]
    tn_o[...] = total[2:4, 0:3]
    flow[6].wait()

    def last(i, _):
        for d in range(2):
            rows = pl.ds(pl.multiple_of(d * 64 + i * 16, 16), 16)
            here = pl.ds(pl.multiple_of(i * 16, 16), 16)
            ig_o[rows, :] = (BASE[rows, :].astype(F32) + RS[d, 6, here, :].astype(F32)).astype(BF16)
        return 0

    lax.fori_loop(0, 4, last, 0)
    tok_last_wait()
    for carrier, sem in sent:
        pltpu.make_async_copy(carrier, carrier, sem).wait()
    assert (next(recv_ids), next(send_ids)) == (N_RECV, N_SEND)


def finish(*refs):
    srcs, dsts, sem = refs[:8], refs[8:16], refs[16]
    copies = [pltpu.make_async_copy(a, b, sem.at[i]) for i, (a, b) in enumerate(zip(srcs, dsts))]
    for c in copies:
        c.start()
    for c in copies:
        c.wait()


def local(tokens, up_gate, up_val, gate_weight, val_weight, gate_taps, val_taps, hidden_grad):
    hbm = pl.BlockSpec(memory_space=pl.ANY)
    half = WIDTH // 2
    scratch = [
        pltpu.VMEM((8, 256, D), BF16),
        pltpu.VMEM((WIDTH, 2 * SEQ), BF16),
        pltpu.VMEM((WIDTH, 2 * SEQ), BF16),
        pltpu.VMEM((WIDTH, 2 * SEQ), BF16),
        pltpu.VMEM((3, WIDTH), BF16),
        pltpu.VMEM((3, WIDTH), BF16),
        pltpu.VMEM((2, WIDTH, 128), F32),
        pltpu.VMEM((2, WIDTH, 128), F32),
        pltpu.VMEM((2 * SEQ, BOTH), BF16),
        pltpu.VMEM((8, BOTH, 256), BF16),
        pltpu.VMEM((4, 4, BOTH, ROWS), BF16),
        pltpu.VMEM((8, BOTH, 256), F32),
        pltpu.VMEM((4, 2, 2, WIDTH, 128), BF16),
        pltpu.VMEM((4, 2, 2, WIDTH, 128), BF16),
        pltpu.VMEM((4, 2, half, 128), BF16),
        pltpu.VMEM((4, 2, half, 128), BF16),
        pltpu.VMEM((2, 2, WIDTH, 128), BF16),
        pltpu.VMEM((2, 2, 2, WIDTH, 128), BF16),
        pltpu.VMEM((2, 2, WIDTH, 128), BF16),
        pltpu.VMEM((2, 2, 2, WIDTH, 128), BF16),
        pltpu.VMEM((2, half, 128), BF16),
        pltpu.VMEM((2, 2, half, 128), BF16),
        pltpu.VMEM((2, half, 128), BF16),
        pltpu.VMEM((2, 2, half, 128), BF16),
        pltpu.VMEM((8, 2, ROWS, D), BF16),
        pltpu.VMEM((8, ROWS, D), BF16),
        pltpu.VMEM((2, 7, 64, D), BF16),
        pltpu.VMEM((4, 2, 8, WIDTH), F32),
        pltpu.VMEM((4, 2, 8, WIDTH), F32),
        pltpu.VMEM((2, 4, 128), F32),
        pltpu.VMEM((8, 4, 128), F32),
        pltpu.VMEM((ROWS, D), BF16),
        pltpu.SemaphoreType.DMA((8,)),
        pltpu.SemaphoreType.DMA((N_SEND,)),
        pltpu.SemaphoreType.DMA((N_RECV,)),
    ]
    shapes = [
        jax.ShapeDtypeStruct((ROWS, D), BF16),
        jax.ShapeDtypeStruct((WIDTH, ROWS), F32),
        jax.ShapeDtypeStruct((WIDTH, ROWS), F32),
        jax.ShapeDtypeStruct((3, WIDTH), F32),
        jax.ShapeDtypeStruct((3, WIDTH), F32),
        jax.ShapeDtypeStruct((1, ROWS), F32),
        jax.ShapeDtypeStruct((1, ROWS), F32),
        jax.ShapeDtypeStruct((2, 3), F32),
    ]
    vmem = pl.BlockSpec(memory_space=pltpu.VMEM)
    args = (
        tokens, up_gate.T, up_val.T, gate_weight.T, val_weight.T, gate_taps, val_taps, hidden_grad.T,
    )
    kept = [pltpu.with_memory_space_constraint(a, pltpu.HBM) for a in args]
    out = pl.pallas_call(
        kernel,
        out_shape=shapes,
        in_specs=[hbm] * 8,
        out_specs=[vmem] * 8,
        scratch_shapes=scratch,
        compiler_params=pltpu.CompilerParams(
            collective_id=0, has_side_effects=True, vmem_limit_bytes=54000000
        ),
        name="backward",
    )(*kept)
    out = pl.pallas_call(
        finish,
        out_shape=shapes,
        in_specs=[vmem] * 8,
        out_specs=[hbm] * 8,
        scratch_shapes=[pltpu.SemaphoreType.DMA((8,))],
        compiler_params=pltpu.CompilerParams(vmem_limit_bytes=4_000_000),
        name="finish",
    )(*out)
    return (out[0], out[1].T, out[2].T, out[3], out[4], out[5].reshape(ROWS), out[6].reshape(ROWS), out[7])


def solution(mesh):
    split = Mesh(mesh.devices.reshape(4, 4, 8, 2), ("y", "x", "z", "c"))
    fs, tp, both = ("y", "x"), ("z", "c"), ("y", "x", "z", "c")
    in_specs = (
        P(both, None), P(fs, tp), P(fs, tp), P(fs, tp), P(fs, tp), P(None, tp), P(None, tp), P(fs, tp),
    )
    out_specs = (
        P(both, None), P(fs, tp), P(fs, tp), P(None, tp), P(None, tp), P(fs), P(fs), P(),
    )
    return jax.shard_map(local, mesh=split, in_specs=in_specs, out_specs=out_specs, check_vma=False)
```
